128 devices in a mesh: sp: 32 (over z, y, core), tp: 4 (over x).
Axes of the slice: x: 4, y: 4, z: 4, core: 2. Of those that a mesh axis runs over, the one named last changes fastest.
Arguments:
- tokens: bfloat16 [4, 2048, 1024], P(None, 'sp', 'tp'), may hold values from -6 to 6
- norm_gain: float32 [4, 1024], replicated, may hold values from 0.1 to 1.9
- val_weight: bfloat16 [4, 1024, 512], P(None, 'sp', 'tp'), may hold values from -0.1875 to 0.1875
- gate_weight: bfloat16 [4, 1024, 512], P(None, 'sp', 'tp'), may hold values from -0.1875 to 0.1875
- conv_taps: float32 [4, 31, 512], P(None, None, 'tp'), may hold values from -1 to 1
- conv_bias: float32 [4, 512], P(None, 'tp'), may hold values from -3 to 3
- ln_gain: float32 [4, 512], P(None, 'tp'), may hold values from 0.1 to 1.9
- ln_shift: float32 [4, 512], P(None, 'tp'), may hold values from -3 to 3
- out_weight: bfloat16 [4, 512, 1024], P(None, 'tp', 'sp'), may hold values from -0.25 to 0.25
Outputs:
- stream: bfloat16 [4, 2048, 1024], P(None, 'sp', 'tp')
The draws below stay inside these ranges and needn't reach their ends.
All inputs are finite; a program needn't handle non-finite values.
Results may differ from the reference program's by a relative error of at most 0.02.
Values may be sent and summed in bfloat16 or wider, within the bound.
No kernel may reach another device: no remote copies, remote signals or barrier semaphores. Data moves between devices by JAX's collectives and lax.ppermute only.
A program may use at most 64 MiB of HBM per device.

```python
import jax
import jax.numpy as jnp
from jax import lax

D = 1024
CHANNELS = 512
TAPS = 31
LAYERS = 4
SEQS = 4
TOKENS = 2048


def level_of(stream_key, dims, shards, low, top_value):
    level = 1.0
    for axis_at, shards_of in shards:
        heights = jax.random.uniform(jax.random.fold_in(jax.random.fold_in(stream_key, 6), axis_at), (shards_of,), jnp.float32, low / len(shards), top_value / len(shards))
        level = level * jnp.repeat(jnp.exp(heights), dims[axis_at] // shards_of).reshape((-1,) + (1,) * (len(dims) - 1 - axis_at))
    return level


def normal_values(own_key, shape, scale, most, shards=(), dtype=jnp.bfloat16):
    result = scale * jax.random.normal(own_key, shape, jnp.float32)
    if shards:
        result = result * level_of(own_key, shape, shards, -0.22, 0.18)
    return jnp.clip(result, -most, most).astype(dtype)


def setup_inputs(seed: int = 0) -> dict:
    splits = jax.random.split(jax.random.key(seed), 10)
    tokens = normal_values(splits[0], (SEQS, TOKENS, D), 1.0, 6.0, ((1, 32), (2, 4)))
    norm_gain = jnp.clip(1.0 + 0.18 * jax.random.normal(splits[1], (LAYERS, D), jnp.float32), 0.1, 1.9)
    val_weight = normal_values(splits[2], (LAYERS, D, CHANNELS), D ** -0.5, 0.1875, ((1, 32), (2, 4)))
    gate_weight = normal_values(splits[3], (LAYERS, D, CHANNELS), D ** -0.5, 0.1875, ((1, 32), (2, 4)))
    conv_taps = normal_values(splits[4], (LAYERS, TAPS, CHANNELS), TAPS ** -0.5, 1.0, ((2, 4),), jnp.float32)
    conv_bias = normal_values(splits[5], (LAYERS, CHANNELS), 0.5, 3.0, ((1, 4),), jnp.float32)
    ln_gain = jnp.clip(1.0 + 0.18 * jax.random.normal(splits[6], (LAYERS, CHANNELS), jnp.float32), 0.1, 1.9)
    ln_shift = normal_values(splits[7], (LAYERS, CHANNELS), 0.5, 3.0, ((1, 4),), jnp.float32)
    out_weight = normal_values(splits[8], (LAYERS, CHANNELS, D), CHANNELS ** -0.5, 0.25, ((1, 4), (2, 32)))
    return {"tokens": tokens, "norm_gain": norm_gain, "val_weight": val_weight, "gate_weight": gate_weight, "conv_taps": conv_taps, "conv_bias": conv_bias, "ln_gain": ln_gain, "ln_shift": ln_shift, "out_weight": out_weight}


epsilon = 1e-06

def depthwise(padded, tap_weights, length):
    running = padded[:, 0:length] * tap_weights[0]
    for tap_idx in range(1, tap_weights.shape[0]):
        running = running + padded[:, tap_idx:tap_idx + length] * tap_weights[tap_idx]
    return running

def reference(tokens, norm_gain, val_weight, gate_weight, conv_taps, conv_bias, ln_gain, ln_shift, out_weight):
    stream = tokens
    half_width = TAPS // 2
    for layer_idx in range(LAYERS):
        widened = stream.astype(jnp.float32)
        scaled = widened * jax.lax.rsqrt(lax.optimization_barrier(jnp.mean(widened * widened, axis=-1, keepdims=True)) + epsilon)
        normed = (scaled * norm_gain[layer_idx]).astype(jnp.bfloat16)
        tok_rows = normed.reshape(-1, D)
        values = jnp.dot(tok_rows, val_weight[layer_idx], preferred_element_type=jnp.float32)
        gates = jnp.dot(tok_rows, gate_weight[layer_idx], preferred_element_type=jnp.float32)
        gated = (values * jax.nn.sigmoid(gates)).astype(jnp.bfloat16).reshape(SEQS, TOKENS, CHANNELS)
        padded = jnp.pad(gated.astype(jnp.float32), ((0, 0), (half_width, half_width), (0, 0)))
        convolved = depthwise(padded, conv_taps[layer_idx], TOKENS) + conv_bias[layer_idx]
        mean_val = lax.optimization_barrier(jnp.mean(convolved, axis=-1, keepdims=True))
        centered = convolved - mean_val
        spread = lax.optimization_barrier(jnp.mean(centered * centered, axis=-1, keepdims=True))
        normalized = centered * jax.lax.rsqrt(spread + epsilon) * ln_gain[layer_idx] + ln_shift[layer_idx]
        activated = jax.nn.silu(normalized).astype(jnp.bfloat16).reshape(-1, CHANNELS)
        branch = jnp.dot(activated, out_weight[layer_idx], preferred_element_type=jnp.float32)
        stream = (stream.astype(jnp.float32) + branch.reshape(SEQS, TOKENS, D)).astype(jnp.bfloat16)
    return stream
```

```python
from functools import partial

import jax
import jax.numpy as jnp
from jax import lax
from jax.experimental import pallas as pl
from jax.experimental.pallas import tpu as pltpu
from jax.sharding import PartitionSpec as P


EPSILON = 1e-06
BF16 = jnp.bfloat16
F32 = jnp.float32
AXES = ("sp", "tp")
LAYERS = 4
HALF = 15
HALO = 64
EDGE = 32


def index_of(z, y, core, x):
    return ((z * 4 + y) * 2 + core) * 4 + x


def place_of(index):
    return index // 32, index // 8 % 4, index // 4 % 2, index % 4


def label(coord, core):
    return (coord + 3 * core) % 4


def coord_of(lab, core):
    return (lab + core) % 4


def swapped(lab, step):
    return lab ^ 1 if step == 0 else 3 - lab


def exchange(axis, step):
    pairs = []
    for device in range(128):
        z, y, core, x = place_of(device)
        at = {"z": z, "y": y, "x": x}
        at[axis] = coord_of(swapped(label(at[axis], core), step), core)
        pairs.append((device, index_of(at["z"], at["y"], core, at["x"])))
    return pairs


def permute(array, pairs):
    return lax.ppermute(array, AXES, pairs)


CORE_SWAP = [(d, d ^ 4) for d in range(128)]
FIRST_STEPS = (("x", 0), ("y", 0), ("z", 0))
LAST_STEPS = (
    (("x", 1), ("y", 1), ("z", 1)),
    (("y", 1), ("z", 1), ("x", 1)),
    (("z", 1), ("x", 1), ("y", 1)),
)


def gather_weights(val_weight, gate_weight, out_weight):
    core = lax.axis_index("sp") % 2
    kinds = jnp.stack([val_weight, gate_weight, jnp.swapaxes(out_weight, 1, 2)])
    lower, upper = kinds[:, :2], kinds[:, 2:]
    mine = jnp.where(core == 0, lower, upper)
    other = permute(jnp.where(core == 0, upper, lower), CORE_SWAP)
    held = jnp.where(
        core == 0, jnp.concatenate([mine, other], axis=2), jnp.concatenate([other, mine], axis=2)
    )[:, None]
    for axis, step in FIRST_STEPS:
        held = jnp.concatenate([held, permute(held, exchange(axis, step))], axis=1)
    colors = [held[k] for k in range(3)]
    for steps in LAST_STEPS[:2]:
        got = [permute(c, exchange(*s)) for c, s in zip(colors, steps)]
        colors = [jnp.concatenate([c, g], axis=0) for c, g in zip(colors, got)]
    got = [permute(c, exchange(*s)) for c, s in zip(colors, LAST_STEPS[2])]
    return [part for c, g in zip(colors, got) for part in (c, g)]


def assemble_kernel(val_a, val_b, gate_a, gate_b, out_a, out_b, w_in, w_out):
    sp, tp = lax.axis_index("sp"), lax.axis_index("tp")
    core = lax.rem(sp, 2)
    chip = lax.div(sp, 2)
    own = {"z": lax.div(chip, 4), "y": lax.rem(chip, 4), "x": tp}
    labels = {a: lax.rem(c + 3 * core, 4) for a, c in own.items()}
    near = {a: {b: l + b - 2 * b * lax.rem(l, 2) for b in (0, 1)} for a, l in labels.items()}
    table = {}
    for a in "zyx":
        for far in (0, 1):
            for b in (0, 1):
                lab = near[a][b]
                lab = 3 - lab if far else lab
                table[a, far, b] = lax.rem(lab + core, 4)
    for color, halves in enumerate(((val_a, val_b), (gate_a, gate_b), (out_a, out_b))):
        order = [LAST_STEPS[s][color][0] for s in range(3)]
        for block in range(64):
            bits = {("x", 0): block & 1, ("y", 0): block >> 1 & 1, ("z", 0): block >> 2 & 1}
            for s, a in enumerate(order):
                bits[a, 1] = block >> (3 + s) & 1
            z, y, x = (table[a, bits[a, 1], bits[a, 0]] for a in "zyx")
            piece = halves[block >> 5][block & 31]
            rows = pl.ds(pl.multiple_of((z * 4 + y) * 64, 64), 64)
            if color == 2:
                w_out[:, rows, pl.ds(pl.multiple_of(x * 128, 128), 128)] = piece
            else:
                w_in[:, rows, pl.ds(pl.multiple_of(color * 512 + x * 128, 128), 128)] = piece


def assemble(parts):
    vmem = pl.BlockSpec(memory_space=pltpu.VMEM)
    return pl.pallas_call(
        assemble_kernel,
        out_shape=(
            jax.ShapeDtypeStruct((2, 1024, 1024), BF16),
            jax.ShapeDtypeStruct((2, 1024, 512), BF16),
        ),
        in_specs=[vmem] * 6,
        out_specs=(vmem, vmem),
        name="assemble",
    )(*parts)


def gather_tokens(tokens):
    tp = lax.axis_index("tp")
    other = permute(tokens, [(d, d ^ 4) for d in range(128) if d & 4])
    both = jnp.concatenate([tokens, other], axis=1)
    columns = [lax.dynamic_index_in_dim(both, tp, 0, keepdims=False)]
    for hop in (1, 2, 3):
        block = lax.dynamic_index_in_dim(both, (tp + hop) % 4, 0, keepdims=False)
        pairs = [(d, d - d % 4 + (d + hop) % 4) for d in range(128) if not d & 4]
        columns.append(permute(block, pairs))
    ordered = [
        lax.select_n((tp - f) % 4, *columns) for f in range(4)
    ]
    middle = jnp.concatenate(ordered, axis=1)
    forward = [(d, d + 8) for d in range(120) if not d & 4]
    backward = [(j, i) for i, j in forward]
    before = permute(middle[128 - HALO :], forward)
    after = permute(middle[:HALO], backward)
    return jnp.concatenate([before, middle, after], axis=0)


def layer(stream, first_token, w_in, w_out, norm_gain, taps, bias, ln_gain, ln_shift):
    rows = stream.shape[0]
    wide = stream.astype(F32)
    scaled = wide * lax.rsqrt(jnp.mean(wide * wide, axis=-1, keepdims=True) + EPSILON)
    normed = (scaled * norm_gain).astype(BF16)
    both = jnp.dot(normed, w_in, preferred_element_type=F32)
    gated = (both[:, :512] * jax.nn.sigmoid(both[:, 512:])).astype(BF16)
    token = first_token + lax.broadcasted_iota(jnp.int32, (rows, 1), 0)
    gated = jnp.where((token >= 0) & (token < 2048), gated, 0).astype(F32)
    padded = jnp.pad(gated, ((HALF, HALF), (0, 0)))
    convolved = padded[0:rows] * taps[0]
    for k in range(1, 31):
        convolved = convolved + padded[k : k + rows] * taps[k]
    convolved = convolved + bias
    mean = jnp.mean(convolved, axis=-1, keepdims=True)
    centered = convolved - mean
    spread = jnp.mean(centered * centered, axis=-1, keepdims=True)
    normalized = centered * lax.rsqrt(spread + EPSILON) * ln_gain + ln_shift
    activated = jax.nn.silu(normalized).astype(BF16)
    branch = lax.dot_general(activated, w_out, (((1,), (1,)), ((), ())), preferred_element_type=F32)
    return (wide + branch).astype(BF16)


def shards(
    tokens, norm_gain, val_weight, gate_weight, conv_taps, conv_bias, ln_gain, ln_shift, out_weight
):
    sp, tp = lax.axis_index("sp"), lax.axis_index("tp")
    core, chip = sp % 2, sp // 2
    small = jnp.concatenate(
        [conv_taps, conv_bias[:, None], ln_gain[:, None], ln_shift[:, None]], axis=1
    )
    small = lax.all_gather(small, "tp", axis=2, tiled=True)
    small = lax.dynamic_slice_in_dim(small, core * 2, 2, 0)
    gains = lax.dynamic_slice_in_dim(norm_gain, core * 2, 2, 0)
    w_in, w_out = assemble(gather_weights(val_weight, gate_weight, out_weight))

    def stage(stream, first_token):
        for l in range(2):
            s = small[l]
            stream = layer(
                stream, first_token, w_in[l], w_out[l], gains[l], s[:31], s[31], s[32], s[33]
            )
        return stream

    stream = stage(gather_tokens(tokens), chip * 128 - HALO)
    stream = permute(stream[EDGE:-EDGE], [(d, d ^ 4) for d in range(128) if not d & 4])
    stream = stage(stream, chip * 128 - HALO + EDGE)
    own = stream[EDGE : EDGE + 128]
    first_half = permute(own[:64], [(d, d ^ 4) for d in range(128) if d & 4])
    mine = jnp.where(core == 1, own[64:], first_half)
    blocks = mine.reshape(64, 4, 256)
    got = [lax.dynamic_index_in_dim(blocks, tp, 1, keepdims=False)]
    for hop in (1, 2, 3):
        block = lax.dynamic_index_in_dim(blocks, (tp + hop) % 4, 1, keepdims=False)
        got.append(permute(block, [(d, d - d % 4 + (d + hop) % 4) for d in range(128)]))
    return jnp.stack([lax.select_n((tp - s) % 4, *got) for s in range(4)])


def solution(mesh):
    return jax.shard_map(
        shards,
        mesh=mesh,
        in_specs=(
            P(None, "sp", "tp"),
            P(),
            P(None, "sp", "tp"),
            P(None, "sp", "tp"),
            P(None, None, "tp"),
            P(None, "tp"),
            P(None, "tp"),
            P(None, "tp"),
            P(None, "tp", "sp"),
        ),
        out_specs=P(None, "sp", "tp"),
        check_vma=False,
    )
```

```python
from functools import partial

import jax
import jax.numpy as jnp
from jax import lax
from jax.experimental import pallas as pl
from jax.experimental.pallas import tpu as pltpu
from jax.sharding import PartitionSpec as P


EPSILON = 1e-06
BF16 = jnp.bfloat16
F32 = jnp.float32
AXES = ("sp", "tp")
LAYERS = 4
HALF = 15
HALO = 64
EDGE = 32


def index_of(z, y, core, x):
    return ((z * 4 + y) * 2 + core) * 4 + x


def place_of(index):
    return index // 32, index // 8 % 4, index // 4 % 2, index % 4


def label(coord, core):
    return (coord + 3 * core) % 4


def coord_of(lab, core):
    return (lab + core) % 4


def swapped(lab, step):
    return lab ^ 1 if step == 0 else 3 - lab


def exchange(axis, step):
    pairs = []
    for device in range(128):
        z, y, core, x = place_of(device)
        at = {"z": z, "y": y, "x": x}
        at[axis] = coord_of(swapped(label(at[axis], core), step), core)
        pairs.append((device, index_of(at["z"], at["y"], core, at["x"])))
    return pairs


def permute(array, pairs):
    return lax.ppermute(array, AXES, pairs)


CORE_SWAP = [(d, d ^ 4) for d in range(128)]
LAST_STEPS = (
    (("x", 1), ("y", 1), ("z", 1)),
    (("y", 1), ("z", 1), ("x", 1)),
    (("z", 1), ("x", 1), ("y", 1)),
)


def block_bits(color):
    order = [LAST_STEPS[s][color][0] for s in range(3)]
    bits = {("x", 0): 0, ("y", 0): 1, ("z", 0): 2}
    bits.update({(axis, 1): 3 + s for s, axis in enumerate(order)})
    return bits


def moves_to(coord, own, core):
    apart = lax.rem(coord + 3 * core, 4) ^ lax.rem(own + 3 * core, 4)
    far = apart >> 1
    return (apart ^ far) & 1, far


def stage_kernel(last, where, *refs):
    if last:
        x_ref, refs = refs[0], refs[1:]
    else:
        before, middle, after, refs = *refs[:3], refs[3:]
    pieces, (par, gain), refs = refs[:12], refs[12:14], refs[14:]
    if last:
        first_out, second_out, refs = refs[0], refs[1], refs[2:]
    else:
        out_ref, refs = refs[0], refs[1:]
    held, stream, normed, gated, conv, act, sems = refs
    z, y, x, core, first_token = (where[i] for i in range(5))
    rows = stream.shape[0]

    def copy(l, k, p):
        return pltpu.make_async_copy(
            pieces[4 * k + p].at[:, l], held.at[k, l, pl.ds(16 * p, 16)], sems.at[l, k, p]
        )

    for l in range(2):
        for k in range(3):
            for p in range(4):
                copy(l, k, p).start()

    if last:
        stream[...] = x_ref[...]
    else:
        for f in range(4):
            near, far = moves_to(f, x, core)
            at = near + 2 * far
            for h in range(2):
                lanes = slice(256 * f + 128 * h, 256 * f + 128 * h + 128)
                stream[0:HALO, lanes] = before[at, h]
                stream[HALO : HALO + 128, lanes] = middle[at, h]
                stream[HALO + 128 :, lanes] = after[at, h]

    zs = [moves_to(i, z, core) for i in range(4)]
    ys = [moves_to(i, y, core) for i in range(4)]

    def block(color, zm, ym, i):
        bits = block_bits(color)
        near, far = i & 1, i >> 1
        fixed = (near << bits["x", 0]) + (far << bits["x", 1])
        return (
            fixed
            + (zm[0] << bits["z", 0])
            + (zm[1] << bits["z", 1])
            + (ym[0] << bits["y", 0])
            + (ym[1] << bits["y", 1])
        )

    token = first_token + lax.broadcasted_iota(jnp.int32, (rows, 128), 0)
    inside = (token >= 0) & (token < 2048)
    gated[0:16, :] = jnp.zeros((16, 512), F32)
    gated[16 + rows :, :] = jnp.zeros((24, 512), F32)

    for l in range(2):
        g = gain[pl.ds(2 * core + l, 1), :]
        for r in range(0, rows, 64):
            wide = stream[r : r + 64, :].astype(F32)
            inv = lax.rsqrt(jnp.mean(wide * wide, axis=-1, keepdims=True) + EPSILON)
            normed[r : r + 64, :] = (wide * inv * g).astype(BF16)
        for k in range(2):
            for p in range(4):
                copy(l, k, p).wait()
        for i in range(4):
            lanes = slice(128 * i, 128 * i + 128)
            w = jnp.concatenate(
                [
                    jnp.concatenate(
                        [held[k, l, block(k, zm, ym, i)] for zm in zs for ym in ys], axis=0
                    )
                    for k in range(2)
                ],
                axis=1,
            )
            both = jnp.dot(normed[...], w, preferred_element_type=F32)
            value = (both[:, :128] * jax.nn.sigmoid(both[:, 128:])).astype(BF16).astype(F32)
            gated[16 : 16 + rows, lanes] = jnp.where(inside, value, 0.0)
        for i in range(4):
            lanes = slice(128 * i, 128 * i + 128)
            taps = [par[l, k : k + 1, lanes] for k in range(31)]
            bias = par[l, 31:32, lanes]
            for r in range(0, rows, 64):
                held_rows = [gated[r + 8 * a : r + 8 * a + 72, lanes] for a in range(4)]
                total = None
                for shift in range(8):
                    part = None
                    for a in range(4):
                        k = 8 * a + shift - 1
                        if k < 0:
                            continue
                        term = held_rows[a] * taps[k]
                        part = term if part is None else part + term
                    part = part[shift : shift + 64]
                    total = part + bias if total is None else total + part
                conv[r : r + 64, lanes] = total
        for r in range(0, rows, 64):
            c = conv[r : r + 64, :]
            mean = jnp.mean(c, axis=-1, keepdims=True)
            c = c - mean
            spread = jnp.mean(c * c, axis=-1, keepdims=True)
            n = c * lax.rsqrt(spread + EPSILON) * par[l, 33:34, :] + par[l, 34:35, :]
            act[r : r + 64, :] = (n * jax.nn.sigmoid(n)).astype(BF16)
        for p in range(4):
            copy(l, 2, p).wait()
        end = last and l == 1
        for q in range(4):
            if end:
                c = lax.rem(x + q, 4)
                zm = moves_to(c, z, core)
                columns = pl.ds(pl.multiple_of(c * 256, 256), 256)
            else:
                zm, columns = zs[q], slice(256 * q, 256 * q + 256)
            w = jnp.concatenate(
                [
                    jnp.concatenate([held[2, l, block(2, zm, ym, i)] for i in range(4)], axis=1)
                    for ym in ys
                ],
                axis=0,
            )
            if end:
                a, s = act[EDGE : EDGE + 128, :], stream[EDGE : EDGE + 128, columns]
            elif l == 1:
                a, s = act[EDGE : rows - EDGE, :], stream[EDGE : rows - EDGE, columns]
            else:
                a, s = act[...], stream[:, columns]
            branch = lax.dot_general(
                a, w, (((1,), (1,)), ((), ())), preferred_element_type=F32
            )
            new = (s.astype(F32) + branch).astype(BF16)
            if end:
                first_out[q] = new[:64]
                second_out[q] = new[64:]
            elif l == 1:
                out_ref[:, columns] = new
            else:
                stream[:, columns] = new


def stage(last, where, inputs, pieces, par, gain):
    vmem = pl.BlockSpec(memory_space=pltpu.VMEM)
    rows = 192 if last else 256
    if last:
        shapes = (jax.ShapeDtypeStruct((4, 64, 256), BF16),) * 2
    else:
        shapes = (jax.ShapeDtypeStruct((192, 1024), BF16),)
    return pl.pallas_call(
        partial(stage_kernel, last),
        out_shape=shapes,
        in_specs=[pl.BlockSpec(memory_space=pltpu.SMEM)]
        + [vmem] * len(inputs)
        + [pl.BlockSpec(memory_space=pl.ANY)] * 12
        + [vmem] * 2,
        out_specs=(vmem,) * len(shapes),
        scratch_shapes=[
            pltpu.VMEM((3, 2, 64, 64, 128), BF16),
            pltpu.VMEM((rows, 1024), BF16),
            pltpu.VMEM((rows, 1024), BF16),
            pltpu.VMEM((16 + rows + 24, 512), F32),
            pltpu.VMEM((rows, 512), F32),
            pltpu.VMEM((rows, 512), BF16),
            pltpu.SemaphoreType.DMA((2, 3, 4)),
        ],
        name="stage_b" if last else "stage_a",
    )(where, *inputs, *pieces, par, gain)


def halves(rows, split):
    return lax.slice_in_dim(rows, 0, split, axis=0), lax.slice_in_dim(rows, split, rows.shape[0], axis=0)


def join(*arrays):
    return jnp.concatenate([a.reshape(-1, 128) for a in arrays], axis=0)


def shards(
    tokens, norm_gain, val_weight, gate_weight, conv_taps, conv_bias, ln_gain, ln_shift, out_weight
):
    sp, tp = lax.axis_index("sp"), lax.axis_index("tp")
    core, chip = sp % 2, sp // 2
    place = lax.rem(tp + 3 * core, 4)

    kinds = jnp.stack([val_weight, gate_weight, jnp.swapaxes(out_weight, 1, 2)])
    lower, upper = kinds[:, :2], kinds[:, 2:]
    mine = jnp.where(core == 0, lower, upper)
    lanes = jnp.stack([tokens[..., :128], tokens[..., 128:]])
    message = join(jnp.where(core == 0, upper, lower), lanes)
    other, other_lanes = halves(permute(message, CORE_SWAP), 192)
    other = other.reshape(3, 2, 32, 128)
    held = jnp.where(
        core == 0, jnp.concatenate([mine, other], axis=2), jnp.concatenate([other, mine], axis=2)
    )
    lanes = jnp.concatenate([lanes, other_lanes.reshape(2, 4, 64, 128)], axis=2)

    small = jnp.concatenate(
        [
            conv_taps,
            conv_bias[:, None],
            jnp.zeros((4, 1, 128), F32),
            ln_gain[:, None],
            ln_shift[:, None],
            jnp.zeros((4, 5, 128), F32),
        ],
        axis=1,
    )
    small = lax.dynamic_slice_in_dim(small, core * 2, 2, 0)
    high = small.astype(BF16)
    params = jnp.stack([high, (small - high.astype(F32)).astype(BF16)])

    def of(lab):
        return lax.dynamic_index_in_dim(lanes, lax.rem((place ^ lab) + core, 4), 1, keepdims=False)

    message = join(held, params, of(1), of(2))
    got, got_small, got_lanes = (
        lambda m: (m[:384].reshape(3, 1, 2, 64, 128), m[384:544], m[544:].reshape(2, 2, 128, 128))
    )(permute(message, exchange("x", 0)))
    held = jnp.concatenate([held[:, None], got], axis=1)
    near_params = jnp.stack([params.reshape(160, 128), got_small])
    keep = jnp.stack([of(0), got_lanes[0]])
    send = jnp.stack([of(3), got_lanes[1]])

    for axis in "yz":
        held = jnp.concatenate([held, permute(held, exchange(axis, 0))], axis=1)

    colors = [held[k] for k in range(3)]
    message = join(colors[0], near_params, send)
    across = permute(message, exchange(*LAST_STEPS[0][0]))
    got = [across[:1024].reshape(8, 2, 64, 128)] + [
        permute(colors[k], exchange(*LAST_STEPS[0][k])) for k in (1, 2)
    ]
    colors = [jnp.concatenate([c, g], axis=0) for c, g in zip(colors, got)]
    far_params = across[1024:1344].reshape(2, 160, 128)
    middle = jnp.concatenate([keep, across[1344:].reshape(2, 2, 128, 128)], axis=0)

    pieces = []
    fifth = [permute(c, exchange(*s)) for c, s in zip(colors, LAST_STEPS[1])]
    sixth = [permute(c, exchange(*s)) for c, s in zip(colors, LAST_STEPS[2])]
    seventh = [permute(c, exchange(*s)) for c, s in zip(fifth, LAST_STEPS[2])]
    for four in zip(colors, fifth, sixth, seventh):
        pieces.extend(four)

    forward = [(d, d + 8) for d in range(120) if not d & 4]
    backward = [(j, i) for i, j in forward]
    before = permute(middle[:, :, 128 - HALO :], forward)
    after = permute(middle[:, :, :HALO], backward)

    both = jnp.concatenate([near_params, far_params], axis=0).reshape(4, 2, 2, 40, 128).astype(F32)
    par = jnp.swapaxes(both[:, 0] + both[:, 1], 0, 1)
    par = jnp.concatenate([par[:, i] for i in range(4)], axis=-1)

    def where(first_token):
        return jnp.stack([chip // 4, chip % 4, tp, core, first_token]).astype(jnp.int32)

    (stream,) = stage(
        False, where(chip * 128 - HALO), (before, middle, after), pieces, par, norm_gain
    )
    stream = permute(stream, [(d, d ^ 4) for d in range(128) if not d & 4])
    first, second = stage(
        True, where(chip * 128 - HALO + EDGE), (stream,), pieces, par, norm_gain
    )
    first = permute(first, [(d, d ^ 4) for d in range(128) if d & 4])
    blocks = jnp.where(core == 1, second, first)
    got = [blocks[0]] + [
        permute(blocks[hop], [(d, d - d % 4 + (d + hop) % 4) for d in range(128)])
        for hop in (1, 2, 3)
    ]
    return jnp.stack([lax.select_n((tp - s) % 4, *got) for s in range(4)])


def solution(mesh):
    return jax.shard_map(
        shards,
        mesh=mesh,
        in_specs=(
            P(None, "sp", "tp"),
            P(),
            P(None, "sp", "tp"),
            P(None, "sp", "tp"),
            P(None, None, "tp"),
            P(None, "tp"),
            P(None, "tp"),
            P(None, "tp"),
            P(None, "tp", "sp"),
        ),
        out_specs=P(None, "sp", "tp"),
        check_vma=False,
    )
```

```python
from functools import partial

import jax
import jax.numpy as jnp
from jax import lax
from jax.experimental import pallas as pl
from jax.experimental.pallas import tpu as pltpu
from jax.sharding import PartitionSpec as P


EPSILON = 1e-06
BF16 = jnp.bfloat16
F32 = jnp.float32
AXES = ("sp", "tp")
LAYERS = 4
HALF = 15
HALO = 64
EDGE = 32


def index_of(z, y, core, x):
    return ((z * 4 + y) * 2 + core) * 4 + x


def place_of(index):
    return index // 32, index // 8 % 4, index // 4 % 2, index % 4


def label(coord, core):
    return (coord + 3 * core) % 4


def coord_of(lab, core):
    return (lab + core) % 4


def swapped(lab, step):
    return lab ^ 1 if step == 0 else 3 - lab


def exchange(axis, step):
    pairs = []
    for device in range(128):
        z, y, core, x = place_of(device)
        at = {"z": z, "y": y, "x": x}
        at[axis] = coord_of(swapped(label(at[axis], core), step), core)
        pairs.append((device, index_of(at["z"], at["y"], core, at["x"])))
    return pairs


def permute(array, pairs):
    return lax.ppermute(array, AXES, pairs)


def nearby(moves):
    pairs = []
    for device in range(128):
        z, y, core, x = place_of(device)
        x, y, z = (
            coord_of(label(c, core) ^ (moves >> i & 1), core) for i, c in enumerate((x, y, z))
        )
        pairs.append((device, index_of(z, y, core, x)))
    return pairs


CORE_SWAP = [(d, d ^ 4) for d in range(128)]
LAST_STEPS = (
    (("x", 1), ("y", 1), ("z", 1)),
    (("y", 1), ("z", 1), ("x", 1)),
    (("z", 1), ("x", 1), ("y", 1)),
)


def block_bits(color):
    order = [LAST_STEPS[s][color][0] for s in range(3)]
    bits = {("x", 0): 0, ("y", 0): 1, ("z", 0): 2}
    bits.update({(axis, 1): 3 + s for s, axis in enumerate(order)})
    return bits


def moves_to(coord, own, core):
    apart = lax.rem(coord + 3 * core, 4) ^ lax.rem(own + 3 * core, 4)
    far = apart >> 1
    return (apart ^ far) & 1, far


def stage_kernel(last, where, *refs):
    pl.when(where[3] == (1 if last else 0))(partial(run_stage, last, where, *refs))


def run_stage(last, where, *refs):
    if last:
        x_ref, refs = refs[0], refs[1:]
    else:
        before, middle, after, refs = *refs[:3], refs[3:]
    pieces, (par, gain), refs = refs[:6], refs[6:8], refs[8:]
    if last:
        first_out, second_out, refs = refs[0], refs[1], refs[2:]
    else:
        out_ref, refs = refs[0], refs[1:]
    stream, normed, gated, conv, act = refs
    z, y, x, core, first_token = (where[i] for i in range(5))
    rows = stream.shape[0]

    def held(color, zm, ym, l, i):
        at = block(color, zm, ym, i)
        if color == 2:
            at = lax.rem(at, 32)
            return jnp.where(ym[1] == 1, pieces[5][at, l], pieces[4][at, l])
        half = zm[1] if color == 0 else i >> 1
        return pieces[2 * color + half][at - 32 * half, l]

    if last:
        stream[...] = x_ref[...]
    else:
        for f in range(4):
            near, far = moves_to(f, x, core)
            at = near + 2 * far
            for h in range(2):
                lanes = slice(256 * f + 128 * h, 256 * f + 128 * h + 128)
                stream[0:HALO, lanes] = before[at, h]
                stream[HALO : HALO + 128, lanes] = middle[at, h]
                stream[HALO + 128 :, lanes] = after[at, h]

    z_moves = [(0, 0), (1, 0), (0, 1), (1, 1)]
    own_z = lax.rem(z + 3 * core, 4)
    z_of = [lax.rem((own_z ^ near ^ 3 * far) + core, 4) for near, far in z_moves]
    zs = [moves_to(i, z, core) for i in range(4)]
    ys = [moves_to(i, y, core) for i in range(4)]

    def block(color, zm, ym, i):
        bits = block_bits(color)
        near, far = i & 1, i >> 1
        fixed = (near << bits["x", 0]) + (far << bits["x", 1])
        return (
            fixed
            + (zm[0] << bits["z", 0])
            + (zm[1] << bits["z", 1])
            + (ym[0] << bits["y", 0])
            + (ym[1] << bits["y", 1])
        )

    token = first_token + lax.broadcasted_iota(jnp.int32, (rows, 128), 0)
    inside = (token >= 0) & (token < 2048)
    gated[0:16, :] = jnp.zeros((16, 512), F32)
    gated[16 + rows :, :] = jnp.zeros((24, 512), F32)

    for l in range(2):
        for r in range(0, rows, 64):
            wide = stream[r : r + 64, :].astype(F32)
            inv = lax.rsqrt(jnp.mean(wide * wide, axis=-1, keepdims=True) + EPSILON)
            for n, c in enumerate(z_of):
                columns = pl.ds(pl.multiple_of(c * 256, 256), 256)
                wide = stream[r : r + 64, columns].astype(F32)
                scaled = wide * inv * gain[pl.ds(2 * core + l, 1), columns]
                normed[r : r + 64, 256 * n : 256 * n + 256] = scaled.astype(BF16)
        for i in range(4):
            lanes = slice(128 * i, 128 * i + 128)
            w = jnp.concatenate(
                [
                    jnp.concatenate(
                        [held(k, zm, ym, l, i) for zm in z_moves for ym in ys], axis=0
                    )
                    for k in range(2)
                ],
                axis=1,
            )
            both = jnp.dot(normed[...], w, preferred_element_type=F32)
            value = (both[:, :128] * jax.nn.sigmoid(both[:, 128:])).astype(BF16).astype(F32)
            gated[16 : 16 + rows, lanes] = jnp.where(inside, value, 0.0)
        for i in range(4):
            lanes = slice(128 * i, 128 * i + 128)
            taps = [par[l, k : k + 1, lanes] for k in range(31)]
            bias = par[l, 31:32, lanes]
            for r in range(0, rows, 64):
                held_rows = [gated[r + 8 * a : r + 8 * a + 72, lanes] for a in range(4)]
                total = None
                for shift in range(8):
                    part = None
                    for a in range(4):
                        k = 8 * a + shift - 1
                        if k < 0:
                            continue
                        term = held_rows[a] * taps[k]
                        part = term if part is None else part + term
                    part = part[shift : shift + 64]
                    total = part + bias if total is None else total + part
                conv[r : r + 64, lanes] = total
        for r in range(0, rows, 64):
            c = conv[r : r + 64, :]
            mean = jnp.mean(c, axis=-1, keepdims=True)
            c = c - mean
            spread = jnp.mean(c * c, axis=-1, keepdims=True)
            n = c * lax.rsqrt(spread + EPSILON) * par[l, 33:34, :] + par[l, 34:35, :]
            act[r : r + 64, :] = (n * jax.nn.sigmoid(n)).astype(BF16)
        end = last and l == 1
        for q in range(4):
            if end:
                c = lax.rem(x + q, 4)
                zm = moves_to(c, z, core)
                columns = pl.ds(pl.multiple_of(c * 256, 256), 256)
            else:
                zm, columns = zs[q], slice(256 * q, 256 * q + 256)
            w = jnp.concatenate(
                [
                    jnp.concatenate([held(2, zm, ym, l, i) for i in range(4)], axis=1)
                    for ym in ys
                ],
                axis=0,
            )
            if end:
                a, s = act[EDGE : EDGE + 128, :], stream[EDGE : EDGE + 128, columns]
            elif l == 1:
                a, s = act[EDGE : rows - EDGE, :], stream[EDGE : rows - EDGE, columns]
            else:
                a, s = act[...], stream[:, columns]
            branch = lax.dot_general(
                a, w, (((1,), (1,)), ((), ())), preferred_element_type=F32
            )
            new = (s.astype(F32) + branch).astype(BF16)
            if end:
                first_out[q] = new[:64]
                second_out[q] = new[64:]
            elif l == 1:
                out_ref[:, columns] = new
            else:
                stream[:, columns] = new


VMEM_BLOCK = pl.BlockSpec(memory_space=pltpu.VMEM)


def vmem(shape, dtype=BF16):
    return pltpu.VMEM(shape, dtype)


def call(kernel, shapes, inputs, name, scalars=None, scratch=(), mib=1):
    operands = [pltpu.with_memory_space_constraint(x, pltpu.VMEM) for x in inputs]
    specs = [VMEM_BLOCK] * len(operands)
    if scalars is not None:
        operands, specs = [scalars] + operands, [pl.BlockSpec(memory_space=pltpu.SMEM)] + specs
    return pl.pallas_call(
        kernel,
        out_shape=shapes,
        in_specs=specs,
        out_specs=(VMEM_BLOCK,) * len(shapes),
        scratch_shapes=scratch,
        compiler_params=pltpu.CompilerParams(vmem_limit_bytes=mib << 20),
        name=name,
    )(*operands)


def stage(last, where, inputs, pieces, par, gain):
    rows = 192 if last else 256
    shapes = (vmem((4, 64, 256)),) * 2 if last else (vmem((192, 1024)),)
    return call(
        partial(stage_kernel, last),
        shapes,
        [*inputs, *pieces, par, gain],
        "stage_b" if last else "stage_a",
        where,
        [
            pltpu.VMEM((rows, 1024), BF16),
            pltpu.VMEM((rows, 1024), BF16),
            pltpu.VMEM((16 + rows + 24, 512), F32),
            pltpu.VMEM((rows, 512), F32),
            pltpu.VMEM((rows, 512), BF16),
        ],
        mib=16,
    )


def begin_kernel(
    where, tokens, val, gate, out, taps, bias, gain, shift, message, mine, lanes, params
):
    core = where[3]
    for k, weight in enumerate((val, gate, out)):
        for l in range(2):
            mine[k, l] = weight[2 * core + l]
            at = 64 * k + 32 * l
            message[at : at + 32] = weight[2 * (1 - core) + l]
    for s in range(4):
        for h in range(2):
            piece = tokens[s, :, 128 * h : 128 * h + 128]
            lanes[h, s] = piece
            at = 192 + 256 * h + 64 * s
            message[at : at + 64] = piece
    for l in range(2):
        layer = 2 * core + l
        for at, ref in ((0, taps), (31, bias), (33, gain), (34, shift)):
            value = ref[layer] if at == 0 else ref[pl.ds(layer, 1)]
            count = 31 if at == 0 else 1
            params[l, at : at + count] = value
        params[l, 32:33] = jnp.zeros((1, 128), F32)
        params[l, 35:40] = jnp.zeros((5, 128), F32)


def begin(where, *inputs):
    shapes = (
        vmem((704, 128)),
        vmem((3, 2, 32, 128)),
        vmem((2, 4, 64, 128)),
        vmem((2, 40, 128), F32),
    )
    return pl.pallas_call(
        begin_kernel,
        out_shape=shapes,
        in_specs=[pl.BlockSpec(memory_space=pltpu.SMEM)] + [VMEM_BLOCK] * len(inputs),
        out_specs=(VMEM_BLOCK,) * 4,
        compiler_params=pltpu.CompilerParams(vmem_limit_bytes=4 << 20),
        name="begin",
    )(where, *inputs)


def meet_kernel(where, mine, lanes, params, other, held, message, keep, across):
    x, core = where[2], where[3]
    label_x = lax.rem(x + 3 * core, 4)
    for k in range(3):
        for l in range(2):
            got = other[64 * k + 32 * l : 64 * k + 32 * l + 32]
            own_rows = pl.ds(pl.multiple_of(32 * core, 32), 32)
            got_rows = pl.ds(pl.multiple_of(32 * (1 - core), 32), 32)
            held[k, l, own_rows] = mine[k, l]
            held[k, l, got_rows] = got
            at = 128 * k + 64 * l
            message[pl.ds(pl.multiple_of(at + 32 * core, 32), 32)] = mine[k, l]
            message[pl.ds(pl.multiple_of(at + 32 * (1 - core), 32), 32)] = got
    for l in range(2):
        p = params[l]
        high = p.astype(BF16)
        low = (p - high.astype(F32)).astype(BF16)
        for target, at in ((message, 384), (across, 0)):
            target[at + 40 * l : at + 40 * l + 40] = high
            target[at + 80 + 40 * l : at + 120 + 40 * l] = low
    for target, at, moves in (
        (keep, 0, 0),
        (message, 544, 1),
        (message, 800, 2),
        (across, 160, 3),
    ):
        s = lax.rem((label_x ^ moves) + core, 4)
        for h in range(2):
            to = at + 128 * h
            target[to : to + 64] = lanes[h, s]
            source = pl.multiple_of(192 + 256 * h + 64 * s, 64)
            target[to + 64 : to + 128] = other[pl.ds(source, 64)]


def meet(where, *inputs):
    shapes = (vmem((3, 2, 64, 128)), vmem((1056, 128)), vmem((256, 128)), vmem((416, 128)))
    return call(meet_kernel, shapes, inputs, "meet", where)


def pack_kernel(held, first, *refs):
    others, (mine, across), (message, col1, col2, keep) = refs[:6], refs[6:8], refs[8:]
    for n in range(8):
        for k in range(3):
            for l in range(2):
                if n == 1:
                    value = first[128 * k + 64 * l : 128 * k + 64 * l + 64]
                else:
                    value = (held if n == 0 else others[n - 2])[k, l]
                if k == 0:
                    message[128 * n + 64 * l : 128 * n + 64 * l + 64] = value
                else:
                    (col1, col2)[k - 1][n, l] = value
    message[1024:1184] = across[0:160]
    message[1184:1344] = first[384:544]
    message[1344:1600] = across[160:416]
    message[1600:1856] = first[800:1056]
    keep[0:256] = mine[...]
    keep[256:512] = first[544:800]


def pack(*inputs):
    return call(
        pack_kernel,
        (vmem((1856, 128)), vmem((8, 2, 64, 128)), vmem((8, 2, 64, 128)), vmem((512, 128))),
        inputs,
        "pack",
    )


def unpack_kernel(keep, own, got, middle, start, end, par):
    for at in range(4):
        for h in range(2):
            for half in range(2):
                source, rows = (keep, 256 * at) if at < 2 else (got, 1344 + 256 * (at - 2))
                rows = rows + 128 * h + 64 * half
                value = source[rows : rows + 64]
                middle[at, h, 64 * half : 64 * half + 64] = value
                (start, end)[half][at, h] = value
        source, rows = (own, 1024 + 160 * at) if at < 2 else (got, 1024 + 160 * (at - 2))
        for l in range(2):
            to = rows + 40 * l
            high, low = source[to : to + 40].astype(F32), source[to + 80 : to + 120].astype(F32)
            par[l, :, 128 * at : 128 * at + 128] = high + low


def unpack(*inputs):
    shapes = (
        vmem((4, 2, 128, 128)),
        vmem((4, 2, 64, 128)),
        vmem((4, 2, 64, 128)),
        vmem((2, 40, 512), F32),
    )
    return call(unpack_kernel, shapes, inputs, "unpack")


def double_kernel(rows, own, got, out):
    out[:rows] = own[:rows]
    out[rows:] = got[:rows]


def double(own, got, blocks):
    own, got = own.reshape(-1, 128), got.reshape(-1, 128)
    rows = blocks * 128
    (out,) = call(partial(double_kernel, rows), (vmem((2 * rows, 128)),), [own, got], "double")
    return out


def finish_kernel(where, own, *refs):
    got, out = refs[:3], refs[3]
    x = where[2]
    out[x] = own[...]
    for hop in (1, 2, 3):
        out[lax.rem(x - hop + 4, 4)] = got[hop - 1][...]


def finish(where, *inputs):
    return pl.pallas_call(
        finish_kernel,
        out_shape=jax.ShapeDtypeStruct((4, 64, 256), BF16),
        in_specs=[pl.BlockSpec(memory_space=pltpu.SMEM)] + [VMEM_BLOCK] * 4,
        out_specs=VMEM_BLOCK,
        compiler_params=pltpu.CompilerParams(vmem_limit_bytes=2 << 20),
        name="finish",
    )(where, *[pltpu.with_memory_space_constraint(i, pltpu.VMEM) for i in inputs])


def shards(
    tokens, norm_gain, val_weight, gate_weight, conv_taps, conv_bias, ln_gain, ln_shift, out_weight
):
    sp, tp = lax.axis_index("sp"), lax.axis_index("tp")
    core, chip = sp % 2, sp // 2

    def where(first_token):
        return jnp.stack([chip // 4, chip % 4, tp, core, first_token]).astype(jnp.int32)

    here = where(chip * 128 - HALO)

    message, mine, lanes, params = begin(
        here,
        tokens,
        val_weight,
        gate_weight,
        jnp.swapaxes(out_weight, 1, 2),
        conv_taps,
        conv_bias,
        ln_gain,
        ln_shift,
    )
    held, message, keep, across = meet(here, mine, lanes, params, permute(message, CORE_SWAP))

    first = permute(message, nearby(1))
    message, *colors, keep = pack(
        held,
        first,
        *[permute(held, nearby(n)) for n in range(2, 8)],
        keep,
        across,
    )

    colors = [message] + colors
    got = [permute(c, exchange(*s)) for c, s in zip(colors, LAST_STEPS[0])]
    middle, start, end, par = unpack(keep, message, got[0])
    colors = [double(c, g, 8) for c, g in zip(colors, got)]
    got = [permute(c, exchange(*s)) for c, s in zip(colors, LAST_STEPS[1])]
    colors = [double(c, g, 16) for c, g in zip(colors, got)]
    got = [permute(c, exchange(*s)) for c, s in zip(colors, LAST_STEPS[2])]
    pieces = [half.reshape(32, 2, 64, 128) for c, g in zip(colors, got) for half in (c, g)]

    forward = [(d, d + 8) for d in range(120) if not d & 4]
    backward = [(j, i) for i, j in forward]
    before = permute(end, forward)
    after = permute(start, backward)

    (stream,) = stage(
        False, here, (before, middle, after), pieces, par, norm_gain
    )
    stream = permute(stream, [(d, d ^ 4) for d in range(128) if not d & 4])
    first, second = stage(
        True, where(chip * 128 - HALO + EDGE), (stream,), pieces, par, norm_gain
    )
    first = permute(first, [(d, d ^ 4) for d in range(128) if d & 4])
    blocks = jnp.where(core == 1, second, first)
    got = [
        permute(blocks[hop], [(d, d - d % 4 + (d + hop) % 4) for d in range(128)])
        for hop in (1, 2, 3)
    ]
    return finish(here, blocks[0], *got)


def solution(mesh):
    return jax.shard_map(
        shards,
        mesh=mesh,
        in_specs=(
            P(None, "sp", "tp"),
            P(),
            P(None, "sp", "tp"),
            P(None, "sp", "tp"),
            P(None, None, "tp"),
            P(None, "tp"),
            P(None, "tp"),
            P(None, "tp"),
            P(None, "tp", "sp"),
        ),
        out_specs=P(None, "sp", "tp"),
        check_vma=False,
    )
```

```python
from functools import partial

import jax
import jax.numpy as jnp
from jax import lax
from jax.experimental import pallas as pl
from jax.experimental.pallas import tpu as pltpu
from jax.sharding import PartitionSpec as P


EPSILON = 1e-06
BF16 = jnp.bfloat16
F32 = jnp.float32
AXES = ("sp", "tp")
LAYERS = 4
HALF = 15
HALO = 64
EDGE = 32


def index_of(z, y, core, x):
    return ((z * 4 + y) * 2 + core) * 4 + x


def place_of(index):
    return index // 32, index // 8 % 4, index // 4 % 2, index % 4


def label(coord, core):
    return (coord + 3 * core) % 4


def coord_of(lab, core):
    return (lab + core) % 4


def swapped(lab, step):
    return lab ^ 1 if step == 0 else 3 - lab


def exchange(axis, step):
    pairs = []
    for device in range(128):
        z, y, core, x = place_of(device)
        at = {"z": z, "y": y, "x": x}
        at[axis] = coord_of(swapped(label(at[axis], core), step), core)
        pairs.append((device, index_of(at["z"], at["y"], core, at["x"])))
    return pairs


def permute(array, pairs):
    return lax.ppermute(array, AXES, pairs)


def nearby(moves):
    pairs = []
    for device in range(128):
        z, y, core, x = place_of(device)
        x, y, z = (
            coord_of(label(c, core) ^ (moves >> i & 1), core) for i, c in enumerate((x, y, z))
        )
        pairs.append((device, index_of(z, y, core, x)))
    return pairs


CORE_SWAP = [(d, d ^ 4) for d in range(128)]
LAST_STEPS = (
    (("x", 1), ("y", 1), ("z", 1)),
    (("y", 1), ("z", 1), ("x", 1)),
    (("z", 1), ("x", 1), ("y", 1)),
)


def block_bits(color):
    order = [LAST_STEPS[s][color][0] for s in range(3)]
    bits = {("x", 0): 0, ("y", 0): 1, ("z", 0): 2}
    bits.update({(axis, 1): 3 + s for s, axis in enumerate(order)})
    return bits


def moves_to(coord, own, core):
    apart = lax.rem(coord + 3 * core, 4) ^ lax.rem(own + 3 * core, 4)
    far = apart >> 1
    return (apart ^ far) & 1, far


def stage_kernel(last, where, *refs):
    pl.when(where[3] == (1 if last else 0))(partial(run_stage, last, where, *refs))


def run_stage(last, where, *refs):
    if last:
        x_ref, refs = refs[0], refs[1:]
    else:
        before, middle, after, refs = *refs[:3], refs[3:]
    pieces, (par, gain), refs = refs[:6], refs[6:8], refs[8:]
    if last:
        first_out, second_out, refs = refs[0], refs[1], refs[2:]
    else:
        out_ref, refs = refs[0], refs[1:]
    stream, normed, gated, conv, act = refs
    z, y, x, core, first_token = (where[i] for i in range(5))
    first_token = first_token + (EDGE if last else 0)
    rows = stream.shape[0]

    def held(color, zm, ym, l, i):
        at = block(color, zm, ym, i)
        if color == 2:
            at = lax.rem(at, 32)
            return jnp.where(ym[1] == 1, pieces[5][at, l], pieces[4][at, l])
        half = zm[1] if color == 0 else i >> 1
        return pieces[2 * color + half][at - 32 * half, l]

    if last:
        stream[...] = x_ref[...]
    else:
        for f in range(4):
            near, far = moves_to(f, x, core)
            at = near + 2 * far
            for h in range(2):
                lanes = slice(256 * f + 128 * h, 256 * f + 128 * h + 128)
                stream[0:HALO, lanes] = before[at, h]
                stream[HALO : HALO + 128, lanes] = middle[at, h]
                stream[HALO + 128 :, lanes] = after[at, h]

    z_moves = [(0, 0), (1, 0), (0, 1), (1, 1)]
    own_z = lax.rem(z + 3 * core, 4)
    z_of = [lax.rem((own_z ^ near ^ 3 * far) + core, 4) for near, far in z_moves]
    zs = [moves_to(i, z, core) for i in range(4)]
    ys = [moves_to(i, y, core) for i in range(4)]

    def block(color, zm, ym, i):
        bits = block_bits(color)
        near, far = i & 1, i >> 1
        fixed = (near << bits["x", 0]) + (far << bits["x", 1])
        return (
            fixed
            + (zm[0] << bits["z", 0])
            + (zm[1] << bits["z", 1])
            + (ym[0] << bits["y", 0])
            + (ym[1] << bits["y", 1])
        )

    token = first_token + lax.broadcasted_iota(jnp.int32, (rows, 128), 0)
    inside = (token >= 0) & (token < 2048)
    gated[0:16, :] = jnp.zeros((16, 512), F32)
    gated[16 + rows :, :] = jnp.zeros((24, 512), F32)

    for l in range(2):
        for r in range(0, rows, 64):
            wide = stream[r : r + 64, :].astype(F32)
            inv = lax.rsqrt(jnp.mean(wide * wide, axis=-1, keepdims=True) + EPSILON)
            for n, c in enumerate(z_of):
                columns = pl.ds(pl.multiple_of(c * 256, 256), 256)
                wide = stream[r : r + 64, columns].astype(F32)
                scaled = wide * inv * gain[pl.ds(2 * core + l, 1), columns]
                normed[r : r + 64, 256 * n : 256 * n + 256] = scaled.astype(BF16)
        for i in range(4):
            lanes = slice(128 * i, 128 * i + 128)
            w = jnp.concatenate(
                [
                    jnp.concatenate(
                        [held(k, zm, ym, l, i) for zm in z_moves for ym in ys], axis=0
                    )
                    for k in range(2)
                ],
                axis=1,
            )
            both = jnp.dot(normed[...], w, preferred_element_type=F32)
            value = (both[:, :128] * jax.nn.sigmoid(both[:, 128:])).astype(BF16).astype(F32)
            gated[16 : 16 + rows, lanes] = jnp.where(inside, value, 0.0)
        for i in range(4):
            lanes = slice(128 * i, 128 * i + 128)
            taps = [par[l, k : k + 1, lanes] for k in range(31)]
            bias = par[l, 31:32, lanes]
            for r in range(0, rows, 64):
                held_rows = [gated[r + 8 * a : r + 8 * a + 72, lanes] for a in range(4)]
                total = None
                for shift in range(8):
                    part = None
                    for a in range(4):
                        k = 8 * a + shift - 1
                        if k < 0:
                            continue
                        term = held_rows[a] * taps[k]
                        part = term if part is None else part + term
                    part = part[shift : shift + 64]
                    total = part + bias if total is None else total + part
                conv[r : r + 64, lanes] = total
        for r in range(0, rows, 64):
            c = conv[r : r + 64, :]
            mean = jnp.mean(c, axis=-1, keepdims=True)
            c = c - mean
            spread = jnp.mean(c * c, axis=-1, keepdims=True)
            n = c * lax.rsqrt(spread + EPSILON) * par[l, 33:34, :] + par[l, 34:35, :]
            act[r : r + 64, :] = (n * jax.nn.sigmoid(n)).astype(BF16)
        end = last and l == 1
        for q in range(4):
            if end:
                c = lax.rem(x + q, 4)
                zm = moves_to(c, z, core)
                columns = pl.ds(pl.multiple_of(c * 256, 256), 256)
            else:
                zm, columns = zs[q], slice(256 * q, 256 * q + 256)
            w = jnp.concatenate(
                [
                    jnp.concatenate([held(2, zm, ym, l, i) for i in range(4)], axis=1)
                    for ym in ys
                ],
                axis=0,
            )
            if end:
                a, s = act[EDGE : EDGE + 128, :], stream[EDGE : EDGE + 128, columns]
            elif l == 1:
                a, s = act[EDGE : rows - EDGE, :], stream[EDGE : rows - EDGE, columns]
            else:
                a, s = act[...], stream[:, columns]
            branch = lax.dot_general(
                a, w, (((1,), (1,)), ((), ())), preferred_element_type=F32
            )
            new = (s.astype(F32) + branch).astype(BF16)
            if end:
                first_out[q] = new[:64]
                second_out[q] = new[64:]
            elif l == 1:
                out_ref[:, columns] = new
            else:
                stream[:, columns] = new


VMEM_BLOCK = pl.BlockSpec(memory_space=pltpu.VMEM)


def vmem(shape, dtype=BF16):
    return pltpu.VMEM(shape, dtype)


def call(kernel, shapes, inputs, name, scalars=None, scratch=(), mib=1):
    operands = [pltpu.with_memory_space_constraint(x, pltpu.VMEM) for x in inputs]
    specs = [VMEM_BLOCK] * len(operands)
    if scalars is not None:
        operands, specs = [scalars] + operands, [pl.BlockSpec(memory_space=pltpu.SMEM)] + specs
    return pl.pallas_call(
        kernel,
        out_shape=shapes,
        in_specs=specs,
        out_specs=(VMEM_BLOCK,) * len(shapes),
        scratch_shapes=scratch,
        compiler_params=pltpu.CompilerParams(vmem_limit_bytes=mib << 20),
        name=name,
    )(*operands)


def stage(last, where, inputs, pieces, par, gain):
    rows = 192 if last else 256
    shapes = (vmem((4, 64, 256)),) * 2 if last else (vmem((192, 1024)),)
    return call(
        partial(stage_kernel, last),
        shapes,
        [*inputs, *pieces, par, gain],
        "stage_b" if last else "stage_a",
        where,
        [
            pltpu.VMEM((rows, 1024), BF16),
            pltpu.VMEM((rows, 1024), BF16),
            pltpu.VMEM((16 + rows + 24, 512), F32),
            pltpu.VMEM((rows, 512), F32),
            pltpu.VMEM((rows, 512), BF16),
        ],
        mib=16,
    )


def begin_kernel(where, tokens, val, gate, out, message, mine, lanes):
    core = where[3]
    for k, weight in enumerate((val, gate, out)):
        for l in range(2):
            mine[k, l] = weight[2 * core + l]
            at = 64 * k + 32 * l
            message[at : at + 32] = weight[2 * (1 - core) + l]
    for s in range(4):
        for h in range(2):
            piece = tokens[s, :, 128 * h : 128 * h + 128]
            lanes[h, s] = piece
            at = 192 + 256 * h + 64 * s
            message[at : at + 64] = piece


def local(kernel, where, inputs, shapes, name):
    return pl.pallas_call(
        kernel,
        out_shape=shapes,
        in_specs=[pl.BlockSpec(memory_space=pltpu.SMEM)] + [VMEM_BLOCK] * len(inputs),
        out_specs=(VMEM_BLOCK,) * len(shapes),
        compiler_params=pltpu.CompilerParams(vmem_limit_bytes=4 << 20),
        name=name,
    )(where, *inputs)


def begin(where, *inputs):
    shapes = (vmem((704, 128)), vmem((3, 2, 32, 128)), vmem((2, 4, 64, 128)))
    return local(begin_kernel, where, inputs, shapes, "begin")


def small_kernel(where, taps, bias, gain, shift, params):
    core = where[3]
    for l in range(2):
        layer = 2 * core + l
        for k in range(31):
            params[l, k : k + 1] = taps[k, pl.ds(layer, 1)]
        params[l, 31:32] = bias[pl.ds(layer, 1)]
        params[l, 32:33] = jnp.zeros((1, 128), F32)
        params[l, 33:34] = gain[pl.ds(layer, 1)]
        params[l, 34:35] = shift[pl.ds(layer, 1)]
        params[l, 35:40] = jnp.zeros((5, 128), F32)


def small(where, *inputs):
    (params,) = local(small_kernel, where, inputs, (vmem((2, 40, 128), F32),), "small")
    return params


def meet_kernel(where, mine, lanes, params, other, held, message, keep, across):
    x, core = where[2], where[3]
    label_x = lax.rem(x + 3 * core, 4)
    for k in range(3):
        for l in range(2):
            got = other[64 * k + 32 * l : 64 * k + 32 * l + 32]
            own_rows = pl.ds(pl.multiple_of(32 * core, 32), 32)
            got_rows = pl.ds(pl.multiple_of(32 * (1 - core), 32), 32)
            held[k, l, own_rows] = mine[k, l]
            held[k, l, got_rows] = got
            at = 128 * k + 64 * l
            message[pl.ds(pl.multiple_of(at + 32 * core, 32), 32)] = mine[k, l]
            message[pl.ds(pl.multiple_of(at + 32 * (1 - core), 32), 32)] = got
    for l in range(2):
        p = params[l]
        high = p.astype(BF16)
        low = (p - high.astype(F32)).astype(BF16)
        for target, at in ((message, 384), (across, 0)):
            target[at + 40 * l : at + 40 * l + 40] = high
            target[at + 80 + 40 * l : at + 120 + 40 * l] = low
    for target, at, moves in (
        (keep, 0, 0),
        (message, 544, 1),
        (message, 800, 2),
        (across, 160, 3),
    ):
        s = lax.rem((label_x ^ moves) + core, 4)
        for h in range(2):
            to = at + 128 * h
            target[to : to + 64] = lanes[h, s]
            source = pl.multiple_of(192 + 256 * h + 64 * s, 64)
            target[to + 64 : to + 128] = other[pl.ds(source, 64)]


def meet(where, *inputs):
    shapes = (vmem((3, 2, 64, 128)), vmem((1056, 128)), vmem((256, 128)), vmem((416, 128)))
    return call(meet_kernel, shapes, inputs, "meet", where)


def pack_kernel(held, first, *refs):
    others, (mine, across), (message, col1, col2, keep) = refs[:6], refs[6:8], refs[8:]
    for n in range(8):
        for k in range(3):
            for l in range(2):
                if n == 1:
                    value = first[128 * k + 64 * l : 128 * k + 64 * l + 64]
                else:
                    value = (held if n == 0 else others[n - 2])[k, l]
                if k == 0:
                    message[128 * n + 64 * l : 128 * n + 64 * l + 64] = value
                else:
                    (col1, col2)[k - 1][n, l] = value
    message[1024:1184] = across[0:160]
    message[1184:1344] = first[384:544]
    message[1344:1600] = across[160:416]
    message[1600:1856] = first[800:1056]
    keep[0:256] = mine[...]
    keep[256:512] = first[544:800]


def pack(*inputs):
    return call(
        pack_kernel,
        (vmem((1856, 128)), vmem((8, 2, 64, 128)), vmem((8, 2, 64, 128)), vmem((512, 128))),
        inputs,
        "pack",
    )


def unpack_kernel(keep, own, got, middle, start, end, par):
    for at in range(4):
        for h in range(2):
            for half in range(2):
                source, rows = (keep, 256 * at) if at < 2 else (got, 1344 + 256 * (at - 2))
                rows = rows + 128 * h + 64 * half
                value = source[rows : rows + 64]
                middle[at, h, 64 * half : 64 * half + 64] = value
                (start, end)[half][at, h] = value
        source, rows = (own, 1024 + 160 * at) if at < 2 else (got, 1024 + 160 * (at - 2))
        for l in range(2):
            to = rows + 40 * l
            high, low = source[to : to + 40].astype(F32), source[to + 80 : to + 120].astype(F32)
            par[l, :, 128 * at : 128 * at + 128] = high + low


def unpack(*inputs):
    shapes = (
        vmem((4, 2, 128, 128)),
        vmem((4, 2, 64, 128)),
        vmem((4, 2, 64, 128)),
        vmem((2, 40, 512), F32),
    )
    return call(unpack_kernel, shapes, inputs, "unpack")


def double_kernel(rows, own, got, out):
    out[:rows] = own[:rows]
    out[rows:] = got[:rows]


def double(own, got, blocks):
    own, got = own.reshape(-1, 128), got.reshape(-1, 128)
    rows = blocks * 128
    (out,) = call(partial(double_kernel, rows), (vmem((2 * rows, 128)),), [own, got], "double")
    return out


def shards(
    tokens, norm_gain, val_weight, gate_weight, conv_taps, conv_bias, ln_gain, ln_shift, out_weight
):
    sp, tp = lax.axis_index("sp"), lax.axis_index("tp")
    core, chip = sp % 2, sp // 2

    here = jnp.stack([chip // 4, chip % 4, tp, core, chip * 128 - HALO]).astype(jnp.int32)

    message, mine, lanes = begin(
        here, tokens, val_weight, gate_weight, jnp.swapaxes(out_weight, 1, 2)
    )
    other = permute(message, CORE_SWAP)
    params = small(here, jnp.swapaxes(conv_taps, 0, 1), conv_bias, ln_gain, ln_shift)
    held, message, keep, across = meet(here, mine, lanes, params, other)

    first = permute(message, nearby(1))
    message, *colors, keep = pack(
        held,
        first,
        *[permute(held, nearby(n)) for n in range(2, 8)],
        keep,
        across,
    )

    colors = [message] + colors
    got = [permute(c, exchange(*s)) for c, s in zip(colors, LAST_STEPS[0])]
    middle, start, end, par = unpack(keep, message, got[0])
    colors = [double(c, g, 8) for c, g in zip(colors, got)]
    got = [permute(c, exchange(*s)) for c, s in zip(colors, LAST_STEPS[1])]
    colors = [double(c, g, 16) for c, g in zip(colors, got)]
    got = [permute(c, exchange(*s)) for c, s in zip(colors, LAST_STEPS[2])]
    pieces = [half.reshape(32, 2, 64, 128) for c, g in zip(colors, got) for half in (c, g)]

    forward = [(d, d + 8) for d in range(120) if not d & 4]
    backward = [(j, i) for i, j in forward]
    before = permute(end, forward)
    after = permute(start, backward)

    (stream,) = stage(
        False, here, (before, middle, after), pieces, par, norm_gain
    )
    stream = permute(stream, [(d, d ^ 4) for d in range(128) if not d & 4])
    first, second = stage(True, here, (stream,), pieces, par, norm_gain)
    first = permute(first, [(d, d ^ 4) for d in range(128) if d & 4])
    blocks = jnp.where(core == 1, second, first)
    got = [blocks[0]] + [
        permute(blocks[hop], [(d, d - d % 4 + (d + hop) % 4) for d in range(128)])
        for hop in (1, 2, 3)
    ]
    return jnp.stack([lax.select_n((tp - s) % 4, *got) for s in range(4)])


def solution(mesh):
    return jax.shard_map(
        shards,
        mesh=mesh,
        in_specs=(
            P(None, "sp", "tp"),
            P(),
            P(None, "sp", "tp"),
            P(None, "sp", "tp"),
            P(None, None, "tp"),
            P(None, "tp"),
            P(None, "tp"),
            P(None, "tp"),
            P(None, "tp", "sp"),
        ),
        out_specs=P(None, "sp", "tp"),
        check_vma=False,
    )
```

```python
from functools import partial

import jax
import jax.numpy as jnp
from jax import lax
from jax.experimental import pallas as pl
from jax.experimental.pallas import tpu as pltpu
from jax.sharding import PartitionSpec as P


EPSILON = 1e-06
BF16 = jnp.bfloat16
F32 = jnp.float32
AXES = ("sp", "tp")
LAYERS = 4
HALF = 15
HALO = 64
EDGE = 32


def index_of(z, y, core, x):
    return ((z * 4 + y) * 2 + core) * 4 + x


def place_of(index):
    return index // 32, index // 8 % 4, index // 4 % 2, index % 4


def label(coord, core):
    return (coord + 3 * core) % 4


def coord_of(lab, core):
    return (lab + core) % 4


def swapped(lab, step):
    return lab ^ 1 if step == 0 else 3 - lab


def exchange(axis, step):
    pairs = []
    for device in range(128):
        z, y, core, x = place_of(device)
        at = {"z": z, "y": y, "x": x}
        at[axis] = coord_of(swapped(label(at[axis], core), step), core)
        pairs.append((device, index_of(at["z"], at["y"], core, at["x"])))
    return pairs


def permute(array, pairs):
    return lax.ppermute(array, AXES, pairs)


def nearby(moves):
    pairs = []
    for device in range(128):
        z, y, core, x = place_of(device)
        x, y, z = (
            coord_of(label(c, core) ^ (moves >> i & 1), core) for i, c in enumerate((x, y, z))
        )
        pairs.append((device, index_of(z, y, core, x)))
    return pairs


CORE_SWAP = [(d, d ^ 4) for d in range(128)]
LAST_STEPS = (
    (("x", 1), ("y", 1), ("z", 1)),
    (("y", 1), ("z", 1), ("x", 1)),
    (("z", 1), ("x", 1), ("y", 1)),
)


def block_bits(color):
    order = [LAST_STEPS[s][color][0] for s in range(3)]
    bits = {("x", 0): 0, ("y", 0): 1, ("z", 0): 2}
    bits.update({(axis, 1): 3 + s for s, axis in enumerate(order)})
    return bits


def moves_to(coord, own, core):
    apart = lax.rem(coord + 3 * core, 4) ^ lax.rem(own + 3 * core, 4)
    far = apart >> 1
    return (apart ^ far) & 1, far


def chunks(low, high):
    return [(r, min(64, high - r)) for r in range(low, high, 64)]


def stage_kernel(last, where, *refs):
    pl.when(where[3] == (1 if last else 0))(partial(run_stage, last, where, *refs))


def run_stage(last, where, *refs):
    if last:
        x_ref, refs = refs[0], refs[1:]
    else:
        before, middle, after, refs = *refs[:3], refs[3:]
    pieces, (par, gain), refs = refs[:6], refs[6:8], refs[8:]
    if last:
        first_out, second_out, refs = refs[0], refs[1], refs[2:]
    else:
        out_ref, refs = refs[0], refs[1:]
    stream, normed, gated, conv, act = refs
    z, y, x, core, first_token = (where[i] for i in range(5))
    first_token = first_token + (EDGE if last else 0)
    rows = stream.shape[0]

    def held(color, zm, ym, l, i):
        at = block(color, zm, ym, i)
        if color == 2:
            at = lax.rem(at, 32)
            return jnp.where(ym[1] == 1, pieces[5][at, l], pieces[4][at, l])
        half = zm[1] if color == 0 else i >> 1
        return pieces[2 * color + half][at - 32 * half, l]

    if last:
        stream[...] = x_ref[...]
    else:
        for f in range(4):
            near, far = moves_to(f, x, core)
            at = near + 2 * far
            for h in range(2):
                lanes = slice(256 * f + 128 * h, 256 * f + 128 * h + 128)
                stream[0:HALO, lanes] = before[at, h]
                stream[HALO : HALO + 128, lanes] = middle[at, h]
                stream[HALO + 128 :, lanes] = after[at, h]

    z_moves = [(0, 0), (1, 0), (0, 1), (1, 1)]
    own_z = lax.rem(z + 3 * core, 4)
    z_of = [lax.rem((own_z ^ near ^ 3 * far) + core, 4) for near, far in z_moves]
    zs = [moves_to(i, z, core) for i in range(4)]
    ys = [moves_to(i, y, core) for i in range(4)]

    def block(color, zm, ym, i):
        bits = block_bits(color)
        near, far = i & 1, i >> 1
        fixed = (near << bits["x", 0]) + (far << bits["x", 1])
        return (
            fixed
            + (zm[0] << bits["z", 0])
            + (zm[1] << bits["z", 1])
            + (ym[0] << bits["y", 0])
            + (ym[1] << bits["y", 1])
        )

    gated[0:16, :] = jnp.zeros((16, 512), F32)
    gated[16 + rows :, :] = jnp.zeros((24, 512), F32)

    for l in range(2):
        low, high = 16 * l, rows - 16 * l
        token = first_token + low + lax.broadcasted_iota(jnp.int32, (high - low, 128), 0)
        inside = (token >= 0) & (token < 2048)
        for r, n_rows in chunks(low, high):
            wide = stream[r : r + n_rows, :].astype(F32)
            inv = lax.rsqrt(jnp.mean(wide * wide, axis=-1, keepdims=True) + EPSILON)
            for n, c in enumerate(z_of):
                columns = pl.ds(pl.multiple_of(c * 256, 256), 256)
                wide = stream[r : r + n_rows, columns].astype(F32)
                scaled = wide * inv * gain[pl.ds(2 * core + l, 1), columns]
                normed[r : r + n_rows, 256 * n : 256 * n + 256] = scaled.astype(BF16)
        for i in range(4):
            lanes = slice(128 * i, 128 * i + 128)
            w = jnp.concatenate(
                [
                    jnp.concatenate(
                        [held(k, zm, ym, l, i) for zm in z_moves for ym in ys], axis=0
                    )
                    for k in range(2)
                ],
                axis=1,
            )
            both = jnp.dot(normed[low:high, :], w, preferred_element_type=F32)
            value = (both[:, :128] * jax.nn.sigmoid(both[:, 128:])).astype(BF16).astype(F32)
            gated[16 + low : 16 + high, lanes] = jnp.where(inside, value, 0.0)
        low, high = low + 16, high - 16
        for i in range(4):
            lanes = slice(128 * i, 128 * i + 128)
            taps = [par[l, k : k + 1, lanes] for k in range(31)]
            bias = par[l, 31:32, lanes]
            for r, n_rows in chunks(low, high):
                held_rows = [
                    gated[r + 8 * a : r + 8 * a + n_rows + 8, lanes] for a in range(4)
                ]
                total = None
                for shift in range(8):
                    part = None
                    for a in range(4):
                        k = 8 * a + shift - 1
                        if k < 0:
                            continue
                        term = held_rows[a] * taps[k]
                        part = term if part is None else part + term
                    part = part[shift : shift + n_rows]
                    total = part + bias if total is None else total + part
                conv[r : r + n_rows, lanes] = total
        for r, n_rows in chunks(low, high):
            c = conv[r : r + n_rows, :]
            mean = jnp.mean(c, axis=-1, keepdims=True)
            c = c - mean
            spread = jnp.mean(c * c, axis=-1, keepdims=True)
            n = c * lax.rsqrt(spread + EPSILON) * par[l, 33:34, :] + par[l, 34:35, :]
            act[r : r + n_rows, :] = (n * jax.nn.sigmoid(n)).astype(BF16)
        end = last and l == 1
        for q in range(4):
            if end:
                c = lax.rem(x + q, 4)
                zm = moves_to(c, z, core)
                columns = pl.ds(pl.multiple_of(c * 256, 256), 256)
            else:
                zm, columns = zs[q], slice(256 * q, 256 * q + 256)
            w = jnp.concatenate(
                [
                    jnp.concatenate([held(2, zm, ym, l, i) for i in range(4)], axis=1)
                    for ym in ys
                ],
                axis=0,
            )
            a, s = act[low:high, :], stream[low:high, columns]
            branch = lax.dot_general(
                a, w, (((1,), (1,)), ((), ())), preferred_element_type=F32
            )
            new = (s.astype(F32) + branch).astype(BF16)
            if end:
                first_out[q] = new[:64]
                second_out[q] = new[64:]
            elif l == 1:
                out_ref[:, columns] = new
            else:
                stream[low:high, columns] = new


VMEM_BLOCK = pl.BlockSpec(memory_space=pltpu.VMEM)


def vmem(shape, dtype=BF16):
    return pltpu.VMEM(shape, dtype)


def call(kernel, shapes, inputs, name, scalars=None, scratch=(), mib=1):
    operands = [pltpu.with_memory_space_constraint(x, pltpu.VMEM) for x in inputs]
    specs = [VMEM_BLOCK] * len(operands)
    if scalars is not None:
        operands, specs = [scalars] + operands, [pl.BlockSpec(memory_space=pltpu.SMEM)] + specs
    return pl.pallas_call(
        kernel,
        out_shape=shapes,
        in_specs=specs,
        out_specs=(VMEM_BLOCK,) * len(shapes),
        scratch_shapes=scratch,
        compiler_params=pltpu.CompilerParams(vmem_limit_bytes=mib << 20),
        name=name,
    )(*operands)


def stage(last, where, inputs, pieces, par, gain):
    rows = 192 if last else 256
    shapes = (vmem((4, 64, 256)),) * 2 if last else (vmem((192, 1024)),)
    return call(
        partial(stage_kernel, last),
        shapes,
        [*inputs, *pieces, par, gain],
        "stage_b" if last else "stage_a",
        where,
        [
            pltpu.VMEM((rows, 1024), BF16),
            pltpu.VMEM((rows, 1024), BF16),
            pltpu.VMEM((16 + rows + 24, 512), F32),
            pltpu.VMEM((rows, 512), F32),
            pltpu.VMEM((rows, 512), BF16),
        ],
        mib=16,
    )


def begin_kernel(where, tokens, val, gate, out, message, mine, lanes):
    core = where[3]
    for k, weight in enumerate((val, gate, out)):
        for l in range(2):
            mine[k, l] = weight[2 * core + l]
            at = 64 * k + 32 * l
            message[at : at + 32] = weight[2 * (1 - core) + l]
    for s in range(4):
        for h in range(2):
            piece = tokens[s, :, 128 * h : 128 * h + 128]
            lanes[h, s] = piece
            at = 192 + 256 * h + 64 * s
            message[at : at + 64] = piece


def local(kernel, where, inputs, shapes, name):
    return pl.pallas_call(
        kernel,
        out_shape=shapes,
        in_specs=[pl.BlockSpec(memory_space=pltpu.SMEM)] + [VMEM_BLOCK] * len(inputs),
        out_specs=(VMEM_BLOCK,) * len(shapes),
        compiler_params=pltpu.CompilerParams(vmem_limit_bytes=4 << 20),
        name=name,
    )(where, *inputs)


def begin(where, *inputs):
    shapes = (vmem((704, 128)), vmem((3, 2, 32, 128)), vmem((2, 4, 64, 128)))
    return local(begin_kernel, where, inputs, shapes, "begin")


def small_kernel(where, taps, bias, gain, shift, params):
    core = where[3]
    for l in range(2):
        layer = 2 * core + l
        for k in range(31):
            params[l, k : k + 1] = taps[k, pl.ds(layer, 1)]
        params[l, 31:32] = bias[pl.ds(layer, 1)]
        params[l, 32:33] = jnp.zeros((1, 128), F32)
        params[l, 33:34] = gain[pl.ds(layer, 1)]
        params[l, 34:35] = shift[pl.ds(layer, 1)]
        params[l, 35:40] = jnp.zeros((5, 128), F32)


def small(where, *inputs):
    (params,) = local(small_kernel, where, inputs, (vmem((2, 40, 128), F32),), "small")
    return params


def meet_kernel(where, mine, lanes, params, other, held, message, keep, across):
    x, core = where[2], where[3]
    label_x = lax.rem(x + 3 * core, 4)
    for k in range(3):
        for l in range(2):
            got = other[64 * k + 32 * l : 64 * k + 32 * l + 32]
            own_rows = pl.ds(pl.multiple_of(32 * core, 32), 32)
            got_rows = pl.ds(pl.multiple_of(32 * (1 - core), 32), 32)
            held[k, l, own_rows] = mine[k, l]
            held[k, l, got_rows] = got
            at = 128 * k + 64 * l
            message[pl.ds(pl.multiple_of(at + 32 * core, 32), 32)] = mine[k, l]
            message[pl.ds(pl.multiple_of(at + 32 * (1 - core), 32), 32)] = got
    for l in range(2):
        p = params[l]
        high = p.astype(BF16)
        low = (p - high.astype(F32)).astype(BF16)
        for target, at in ((message, 384), (across, 0)):
            target[at + 40 * l : at + 40 * l + 40] = high
            target[at + 80 + 40 * l : at + 120 + 40 * l] = low
    for target, at, moves in (
        (keep, 0, 0),
        (message, 544, 1),
        (message, 800, 2),
        (across, 160, 3),
    ):
        s = lax.rem((label_x ^ moves) + core, 4)
        for h in range(2):
            to = at + 128 * h
            target[to : to + 64] = lanes[h, s]
            source = pl.multiple_of(192 + 256 * h + 64 * s, 64)
            target[to + 64 : to + 128] = other[pl.ds(source, 64)]


def meet(where, *inputs):
    shapes = (vmem((3, 2, 64, 128)), vmem((1056, 128)), vmem((256, 128)), vmem((416, 128)))
    return call(meet_kernel, shapes, inputs, "meet", where)


def pack_kernel(held, first, *refs):
    others, (mine, across), (message, col1, col2, keep) = refs[:6], refs[6:8], refs[8:]
    for n in range(8):
        for k in range(3):
            for l in range(2):
                if n == 1:
                    value = first[128 * k + 64 * l : 128 * k + 64 * l + 64]
                else:
                    value = (held if n == 0 else others[n - 2])[k, l]
                if k == 0:
                    message[128 * n + 64 * l : 128 * n + 64 * l + 64] = value
                else:
                    (col1, col2)[k - 1][n, l] = value
    message[1024:1184] = across[0:160]
    message[1184:1344] = first[384:544]
    message[1344:1600] = across[160:416]
    message[1600:1856] = first[800:1056]
    keep[0:256] = mine[...]
    keep[256:512] = first[544:800]


def pack(*inputs):
    return call(
        pack_kernel,
        (vmem((1856, 128)), vmem((8, 2, 64, 128)), vmem((8, 2, 64, 128)), vmem((512, 128))),
        inputs,
        "pack",
    )


def unpack_kernel(keep, own, got, middle, start, end, par):
    for at in range(4):
        for h in range(2):
            for half in range(2):
                source, rows = (keep, 256 * at) if at < 2 else (got, 1344 + 256 * (at - 2))
                rows = rows + 128 * h + 64 * half
                value = source[rows : rows + 64]
                middle[at, h, 64 * half : 64 * half + 64] = value
                (start, end)[half][at, h] = value
        source, rows = (own, 1024 + 160 * at) if at < 2 else (got, 1024 + 160 * (at - 2))
        for l in range(2):
            to = rows + 40 * l
            high, low = source[to : to + 40].astype(F32), source[to + 80 : to + 120].astype(F32)
            par[l, :, 128 * at : 128 * at + 128] = high + low


def unpack(*inputs):
    shapes = (
        vmem((4, 2, 128, 128)),
        vmem((4, 2, 64, 128)),
        vmem((4, 2, 64, 128)),
        vmem((2, 40, 512), F32),
    )
    return call(unpack_kernel, shapes, inputs, "unpack")


def double_kernel(rows, own, got, out):
    out[:rows] = own[:rows]
    out[rows:] = got[:rows]


def double(own, got, blocks):
    own, got = own.reshape(-1, 128), got.reshape(-1, 128)
    rows = blocks * 128
    (out,) = call(partial(double_kernel, rows), (vmem((2 * rows, 128)),), [own, got], "double")
    return out


def shards(
    tokens, norm_gain, val_weight, gate_weight, conv_taps, conv_bias, ln_gain, ln_shift, out_weight
):
    sp, tp = lax.axis_index("sp"), lax.axis_index("tp")
    core, chip = sp % 2, sp // 2

    here = jnp.stack([chip // 4, chip % 4, tp, core, chip * 128 - HALO]).astype(jnp.int32)

    message, mine, lanes = begin(
        here, tokens, val_weight, gate_weight, jnp.swapaxes(out_weight, 1, 2)
    )
    other = permute(message, CORE_SWAP)
    params = small(here, jnp.swapaxes(conv_taps, 0, 1), conv_bias, ln_gain, ln_shift)
    held, message, keep, across = meet(here, mine, lanes, params, other)

    first = permute(message, nearby(1))
    message, *colors, keep = pack(
        held,
        first,
        *[permute(held, nearby(n)) for n in range(2, 8)],
        keep,
        across,
    )

    colors = [message] + colors
    got = [permute(c, exchange(*s)) for c, s in zip(colors, LAST_STEPS[0])]
    middle, start, end, par = unpack(keep, message, got[0])
    colors = [double(c, g, 8) for c, g in zip(colors, got)]
    got = [permute(c, exchange(*s)) for c, s in zip(colors, LAST_STEPS[1])]
    colors = [double(c, g, 16) for c, g in zip(colors, got)]
    got = [permute(c, exchange(*s)) for c, s in zip(colors, LAST_STEPS[2])]
    pieces = [half.reshape(32, 2, 64, 128) for c, g in zip(colors, got) for half in (c, g)]

    forward = [(d, d + 8) for d in range(120) if not d & 4]
    backward = [(j, i) for i, j in forward]
    before = permute(end, forward)
    after = permute(start, backward)

    (stream,) = stage(
        False, here, (before, middle, after), pieces, par, norm_gain
    )
    stream = permute(stream, [(d, d ^ 4) for d in range(128) if not d & 4])
    first, second = stage(True, here, (stream,), pieces, par, norm_gain)
    first = permute(first, [(d, d ^ 4) for d in range(128) if d & 4])
    blocks = jnp.where(core == 1, second, first)
    got = [blocks[0]] + [
        permute(blocks[hop], [(d, d - d % 4 + (d + hop) % 4) for d in range(128)])
        for hop in (1, 2, 3)
    ]
    return jnp.stack([lax.select_n((tp - s) % 4, *got) for s in range(4)])


def solution(mesh):
    return jax.shard_map(
        shards,
        mesh=mesh,
        in_specs=(
            P(None, "sp", "tp"),
            P(),
            P(None, "sp", "tp"),
            P(None, "sp", "tp"),
            P(None, None, "tp"),
            P(None, "tp"),
            P(None, "tp"),
            P(None, "tp"),
            P(None, "tp", "sp"),
        ),
        out_specs=P(None, "sp", "tp"),
        check_vma=False,
    )
```

```python
from functools import partial

import jax
import jax.numpy as jnp
from jax import lax
from jax.experimental import pallas as pl
from jax.experimental.pallas import tpu as pltpu
from jax.sharding import PartitionSpec as P


EPSILON = 1e-06
BF16 = jnp.bfloat16
F32 = jnp.float32
AXES = ("sp", "tp")
LAYERS = 4
HALF = 15
HALO = 64
EDGE = 32


def index_of(z, y, core, x):
    return ((z * 4 + y) * 2 + core) * 4 + x


def place_of(index):
    return index // 32, index // 8 % 4, index // 4 % 2, index % 4


def label(coord, core):
    return (coord + 3 * core) % 4


def coord_of(lab, core):
    return (lab + core) % 4


def swapped(lab, step):
    return lab ^ 1 if step == 0 else 3 - lab


def exchange(axis, step):
    pairs = []
    for device in range(128):
        z, y, core, x = place_of(device)
        at = {"z": z, "y": y, "x": x}
        at[axis] = coord_of(swapped(label(at[axis], core), step), core)
        pairs.append((device, index_of(at["z"], at["y"], core, at["x"])))
    return pairs


def permute(array, pairs):
    return lax.ppermute(array, AXES, pairs)


def nearby(moves):
    pairs = []
    for device in range(128):
        z, y, core, x = place_of(device)
        x, y, z = (
            coord_of(label(c, core) ^ (moves >> i & 1), core) for i, c in enumerate((x, y, z))
        )
        pairs.append((device, index_of(z, y, core, x)))
    return pairs


CORE_SWAP = [(d, d ^ 4) for d in range(128)]
LAST_STEPS = (
    (("x", 1), ("y", 1), ("z", 1)),
    (("y", 1), ("z", 1), ("x", 1)),
    (("z", 1), ("x", 1), ("y", 1)),
)


def block_bits(color):
    order = [LAST_STEPS[s][color][0] for s in range(3)]
    bits = {("x", 0): 0, ("y", 0): 1, ("z", 0): 2}
    bits.update({(axis, 1): 3 + s for s, axis in enumerate(order)})
    return bits


def moves_to(coord, own, core):
    apart = lax.rem(coord + 3 * core, 4) ^ lax.rem(own + 3 * core, 4)
    far = apart >> 1
    return (apart ^ far) & 1, far


def chunks(low, high):
    return [(r, min(64, high - r)) for r in range(low, high, 64)]


def stage_kernel(last, where, *refs):
    pl.when(where[3] == (1 if last else 0))(partial(run_stage, last, where, *refs))


def run_stage(last, where, *refs):
    if last:
        x_ref, refs = refs[0], refs[1:]
    else:
        before, middle, after, refs = *refs[:3], refs[3:]
    pieces, (par, gain), refs = refs[:6], refs[6:8], refs[8:]
    if last:
        first_out, second_out, refs = refs[0], refs[1], refs[2:]
    else:
        out_ref, refs = refs[0], refs[1:]
    stream, normed, gated, conv, act = refs
    z, y, x, core, first_token = (where[i] for i in range(5))
    first_token = first_token + (EDGE if last else 0)
    rows = stream.shape[0]

    def held(color, zm, ym, l, i):
        at = block(color, zm, ym, i)
        if color == 2:
            at = lax.rem(at, 32)
            return jnp.where(ym[1] == 1, pieces[5][at, l], pieces[4][at, l])
        half = zm[1] if color == 0 else i >> 1
        return pieces[2 * color + half][at - 32 * half, l]

    if last:
        stream[...] = x_ref[...]
    else:
        for f in range(4):
            near, far = moves_to(f, x, core)
            at = near + 2 * far
            for h in range(2):
                lanes = slice(256 * f + 128 * h, 256 * f + 128 * h + 128)
                stream[0:HALO, lanes] = before[at, h]
                stream[HALO : HALO + 128, lanes] = middle[at, h]
                stream[HALO + 128 :, lanes] = after[at, h]

    z_moves = [(0, 0), (1, 0), (0, 1), (1, 1)]
    own_z = lax.rem(z + 3 * core, 4)
    z_of = [lax.rem((own_z ^ near ^ 3 * far) + core, 4) for near, far in z_moves]
    zs = [moves_to(i, z, core) for i in range(4)]
    ys = [moves_to(i, y, core) for i in range(4)]

    def block(color, zm, ym, i):
        bits = block_bits(color)
        near, far = i & 1, i >> 1
        fixed = (near << bits["x", 0]) + (far << bits["x", 1])
        return (
            fixed
            + (zm[0] << bits["z", 0])
            + (zm[1] << bits["z", 1])
            + (ym[0] << bits["y", 0])
            + (ym[1] << bits["y", 1])
        )

    gated[0:16, :] = jnp.zeros((16, 512), F32)
    gated[16 + rows :, :] = jnp.zeros((24, 512), F32)

    for l in range(2):
        low, high = 16 * l, rows - 16 * l
        token = first_token + low + lax.broadcasted_iota(jnp.int32, (high - low, 128), 0)
        inside = (token >= 0) & (token < 2048)
        for r, n_rows in chunks(low, high):
            wide = stream[r : r + n_rows, :].astype(F32)
            inv = lax.rsqrt(jnp.mean(wide * wide, axis=-1, keepdims=True) + EPSILON)
            for n, c in enumerate(z_of):
                columns = pl.ds(pl.multiple_of(c * 256, 256), 256)
                wide = stream[r : r + n_rows, columns].astype(F32)
                scaled = wide * inv * gain[pl.ds(2 * core + l, 1), columns]
                normed[r : r + n_rows, 256 * n : 256 * n + 256] = scaled.astype(BF16)
        for i in range(4):
            lanes = slice(128 * i, 128 * i + 128)
            w = jnp.concatenate(
                [
                    jnp.concatenate(
                        [held(k, zm, ym, l, i) for zm in z_moves for ym in ys], axis=0
                    )
                    for k in range(2)
                ],
                axis=1,
            )
            both = jnp.dot(normed[low:high, :], w, preferred_element_type=F32)
            value = (both[:, :128] * jax.nn.sigmoid(both[:, 128:])).astype(BF16).astype(F32)
            gated[16 + low : 16 + high, lanes] = jnp.where(inside, value, 0.0)
        low, high = low + 16, high - 16
        for i in range(4):
            lanes = slice(128 * i, 128 * i + 128)
            taps = [par[l, k : k + 1, lanes] for k in range(31)]
            bias = par[l, 31:32, lanes]
            for r, n_rows in chunks(low, high):
                held_rows = [
                    gated[r + 8 * a : r + 8 * a + n_rows + 8, lanes] for a in range(4)
                ]
                total = None
                for shift in range(8):
                    part = None
                    for a in range(4):
                        k = 8 * a + shift - 1
                        if k < 0:
                            continue
                        term = held_rows[a] * taps[k]
                        part = term if part is None else part + term
                    part = part[shift : shift + n_rows]
                    total = part + bias if total is None else total + part
                conv[r : r + n_rows, lanes] = total
        for r, n_rows in chunks(low, high):
            c = conv[r : r + n_rows, :]
            mean = jnp.mean(c, axis=-1, keepdims=True)
            c = c - mean
            spread = jnp.mean(c * c, axis=-1, keepdims=True)
            n = c * lax.rsqrt(spread + EPSILON) * par[l, 33:34, :] + par[l, 34:35, :]
            act[r : r + n_rows, :] = (n * jax.nn.sigmoid(n)).astype(BF16)
        end = last and l == 1
        for q in range(4):
            if end:
                c = lax.rem(x + q, 4)
                zm = moves_to(c, z, core)
                columns = pl.ds(pl.multiple_of(c * 256, 256), 256)
            else:
                zm, columns = zs[q], slice(256 * q, 256 * q + 256)
            w = jnp.concatenate(
                [
                    jnp.concatenate([held(2, zm, ym, l, i) for i in range(4)], axis=1)
                    for ym in ys
                ],
                axis=0,
            )
            a, s = act[low:high, :], stream[low:high, columns]
            branch = lax.dot_general(
                a, w, (((1,), (1,)), ((), ())), preferred_element_type=F32
            )
            new = (s.astype(F32) + branch).astype(BF16)
            if end:
                first_out[q] = new[:64]
                second_out[q] = new[64:]
            elif l == 1:
                out_ref[:, columns] = new
            else:
                stream[low:high, columns] = new


VMEM_BLOCK = pl.BlockSpec(memory_space=pltpu.VMEM)


def vmem(shape, dtype=BF16):
    return pltpu.VMEM(shape, dtype)


def call(kernel, shapes, inputs, name, scalars=None, scratch=(), mib=1):
    operands = [pltpu.with_memory_space_constraint(x, pltpu.VMEM) for x in inputs]
    specs = [VMEM_BLOCK] * len(operands)
    if scalars is not None:
        operands, specs = [scalars] + operands, [pl.BlockSpec(memory_space=pltpu.SMEM)] + specs
    return pl.pallas_call(
        kernel,
        out_shape=shapes,
        in_specs=specs,
        out_specs=(VMEM_BLOCK,) * len(shapes),
        scratch_shapes=scratch,
        compiler_params=pltpu.CompilerParams(vmem_limit_bytes=mib << 20),
        name=name,
    )(*operands)


def stage(last, where, inputs, pieces, par, gain):
    rows = 192 if last else 256
    shapes = (vmem((4, 64, 256)),) * 2 if last else (vmem((192, 1024)),)
    return call(
        partial(stage_kernel, last),
        shapes,
        [*inputs, *pieces, par, gain],
        "stage_b" if last else "stage_a",
        where,
        [
            pltpu.VMEM((rows, 1024), BF16),
            pltpu.VMEM((rows, 1024), BF16),
            pltpu.VMEM((16 + rows + 24, 512), F32),
            pltpu.VMEM((rows, 512), F32),
            pltpu.VMEM((rows, 512), BF16),
        ],
        mib=16,
    )


def begin_kernel(where, tokens, val, gate, out, message, mine, lanes):
    core = where[3]
    for k, weight in enumerate((val, gate, out)):
        for l in range(2):
            mine[k, l] = weight[2 * core + l]
            at = 64 * k + 32 * l
            message[at : at + 32] = weight[2 * (1 - core) + l]
    for s in range(4):
        for h in range(2):
            piece = tokens[s, :, 128 * h : 128 * h + 128]
            lanes[h, s] = piece
            at = 192 + 256 * h + 64 * s
            message[at : at + 64] = piece


def local(kernel, where, inputs, shapes, name):
    return pl.pallas_call(
        kernel,
        out_shape=shapes,
        in_specs=[pl.BlockSpec(memory_space=pltpu.SMEM)] + [VMEM_BLOCK] * len(inputs),
        out_specs=(VMEM_BLOCK,) * len(shapes),
        compiler_params=pltpu.CompilerParams(vmem_limit_bytes=4 << 20),
        name=name,
    )(where, *inputs)


def begin(where, *inputs):
    shapes = (vmem((704, 128)), vmem((3, 2, 32, 128)), vmem((2, 4, 64, 128)))
    return local(begin_kernel, where, inputs, shapes, "begin")


def small_kernel(where, taps, bias, gain, shift, params):
    core = where[3]
    for l in range(2):
        layer = 2 * core + l
        for k in range(31):
            params[l, k : k + 1] = taps[k, pl.ds(layer, 1)]
        params[l, 31:32] = bias[pl.ds(layer, 1)]
        params[l, 32:33] = jnp.zeros((1, 128), F32)
        params[l, 33:34] = gain[pl.ds(layer, 1)]
        params[l, 34:35] = shift[pl.ds(layer, 1)]
        params[l, 35:40] = jnp.zeros((5, 128), F32)


def small(where, *inputs):
    (params,) = local(small_kernel, where, inputs, (vmem((2, 40, 128), F32),), "small")
    return params


def meet_kernel(where, mine, lanes, params, other, held, message, keep, across):
    x, core = where[2], where[3]
    label_x = lax.rem(x + 3 * core, 4)
    for k in range(3):
        for l in range(2):
            got = other[64 * k + 32 * l : 64 * k + 32 * l + 32]
            own_rows = pl.ds(pl.multiple_of(32 * core, 32), 32)
            got_rows = pl.ds(pl.multiple_of(32 * (1 - core), 32), 32)
            held[k, l, own_rows] = mine[k, l]
            held[k, l, got_rows] = got
            at = 128 * k + 64 * l
            message[pl.ds(pl.multiple_of(at + 32 * core, 32), 32)] = mine[k, l]
            message[pl.ds(pl.multiple_of(at + 32 * (1 - core), 32), 32)] = got
    for l in range(2):
        p = params[l]
        high = p.astype(BF16)
        low = (p - high.astype(F32)).astype(BF16)
        for target, at in ((message, 384), (across, 0)):
            target[at + 40 * l : at + 40 * l + 40] = high
            target[at + 80 + 40 * l : at + 120 + 40 * l] = low
    for target, at, moves in (
        (keep, 0, 0),
        (message, 544, 1),
        (message, 800, 2),
        (across, 160, 3),
    ):
        s = lax.rem((label_x ^ moves) + core, 4)
        for h in range(2):
            to = at + 128 * h
            target[to : to + 64] = lanes[h, s]
            source = pl.multiple_of(192 + 256 * h + 64 * s, 64)
            target[to + 64 : to + 128] = other[pl.ds(source, 64)]


def meet(where, *inputs):
    shapes = (vmem((3, 2, 64, 128)), vmem((1056, 128)), vmem((256, 128)), vmem((416, 128)))
    return call(meet_kernel, shapes, inputs, "meet", where)


def pack_kernel(held, first, *refs):
    others, (mine, across), (message, col1, col2, keep) = refs[:6], refs[6:8], refs[8:]
    for n in range(8):
        for k in range(3):
            for l in range(2):
                if n == 1:
                    value = first[128 * k + 64 * l : 128 * k + 64 * l + 64]
                else:
                    value = (held if n == 0 else others[7 - n])[k, l]
                if k == 0:
                    message[128 * n + 64 * l : 128 * n + 64 * l + 64] = value
                else:
                    (col1, col2)[k - 1][n, l] = value
    message[1024:1184] = across[0:160]
    message[1184:1344] = first[384:544]
    message[1344:1600] = across[160:416]
    message[1600:1856] = first[800:1056]
    keep[0:256] = mine[...]
    keep[256:512] = first[544:800]


def pack(*inputs):
    return call(
        pack_kernel,
        (vmem((1856, 128)), vmem((8, 2, 64, 128)), vmem((8, 2, 64, 128)), vmem((512, 128))),
        inputs,
        "pack",
    )


def unpack_kernel(keep, own, got, middle, start, end, par):
    for at in range(4):
        for h in range(2):
            for half in range(2):
                source, rows = (keep, 256 * at) if at < 2 else (got, 1344 + 256 * (at - 2))
                rows = rows + 128 * h + 64 * half
                value = source[rows : rows + 64]
                middle[at, h, 64 * half : 64 * half + 64] = value
                (start, end)[half][at, h] = value
        source, rows = (own, 1024 + 160 * at) if at < 2 else (got, 1024 + 160 * (at - 2))
        for l in range(2):
            to = rows + 40 * l
            high, low = source[to : to + 40].astype(F32), source[to + 80 : to + 120].astype(F32)
            par[l, :, 128 * at : 128 * at + 128] = high + low


def unpack(*inputs):
    shapes = (
        vmem((4, 2, 128, 128)),
        vmem((4, 2, 64, 128)),
        vmem((4, 2, 64, 128)),
        vmem((2, 40, 512), F32),
    )
    return call(unpack_kernel, shapes, inputs, "unpack")


def double_kernel(rows, own, got, out):
    out[:rows] = own[:rows]
    out[rows:] = got[:rows]


def double(own, got, blocks):
    own, got = own.reshape(-1, 128), got.reshape(-1, 128)
    rows = blocks * 128
    (out,) = call(partial(double_kernel, rows), (vmem((2 * rows, 128)),), [own, got], "double")
    return out


def shards(
    tokens, norm_gain, val_weight, gate_weight, conv_taps, conv_bias, ln_gain, ln_shift, out_weight
):
    sp, tp = lax.axis_index("sp"), lax.axis_index("tp")
    core, chip = sp % 2, sp // 2

    here = jnp.stack([chip // 4, chip % 4, tp, core, chip * 128 - HALO]).astype(jnp.int32)

    message, mine, lanes = begin(
        here, tokens, val_weight, gate_weight, jnp.swapaxes(out_weight, 1, 2)
    )
    other = permute(message, CORE_SWAP)
    params = small(here, jnp.swapaxes(conv_taps, 0, 1), conv_bias, ln_gain, ln_shift)
    held, message, keep, across = meet(here, mine, lanes, params, other)

    first = permute(message, nearby(1))
    others = [permute(held, nearby(n)) for n in (7, 6, 5, 4, 3, 2)]
    message, *colors, keep = pack(
        held,
        first,
        *others,
        keep,
        across,
    )

    colors = [message] + colors
    got = [permute(c, exchange(*s)) for c, s in zip(colors, LAST_STEPS[0])]
    middle, start, end, par = unpack(keep, message, got[0])
    colors = [double(c, g, 8) for c, g in zip(colors, got)]
    got = [permute(c, exchange(*s)) for c, s in zip(colors, LAST_STEPS[1])]
    colors = [double(c, g, 16) for c, g in zip(colors, got)]
    got = [permute(c, exchange(*s)) for c, s in zip(colors, LAST_STEPS[2])]
    pieces = [half.reshape(32, 2, 64, 128) for c, g in zip(colors, got) for half in (c, g)]

    forward = [(d, d + 8) for d in range(120) if not d & 4]
    backward = [(j, i) for i, j in forward]
    before = permute(end, forward)
    after = permute(start, backward)

    (stream,) = stage(
        False, here, (before, middle, after), pieces, par, norm_gain
    )
    stream = permute(stream, [(d, d ^ 4) for d in range(128) if not d & 4])
    first, second = stage(True, here, (stream,), pieces, par, norm_gain)
    first = permute(first, [(d, d ^ 4) for d in range(128) if d & 4])
    blocks = jnp.where(core == 1, second, first)
    got = [blocks[0]] + [
        permute(blocks[hop], [(d, d - d % 4 + (d + hop) % 4) for d in range(128)])
        for hop in (1, 2, 3)
    ]
    return jnp.stack([lax.select_n((tp - s) % 4, *got) for s in range(4)])


def solution(mesh):
    return jax.shard_map(
        shards,
        mesh=mesh,
        in_specs=(
            P(None, "sp", "tp"),
            P(),
            P(None, "sp", "tp"),
            P(None, "sp", "tp"),
            P(None, None, "tp"),
            P(None, "tp"),
            P(None, "tp"),
            P(None, "tp"),
            P(None, "tp", "sp"),
        ),
        out_specs=P(None, "sp", "tp"),
        check_vma=False,
    )
```
